32 devices in a mesh: ep: 16 (over z, x, core), tp: 2 (over y).
Axes of the slice: x: 2, y: 2, z: 4, core: 2. Of those that a mesh axis runs over, the one named last changes fastest.
Arguments:
- tokens: bfloat16 [192, 4096], P('ep', 'tp')
- norm_gain: float32 [4096], P('tp'), may hold values from 0.1 to 1.9
- routes: int32 [192, 6], P('ep'), may hold values from 0 to 15, all different within a row; in each aligned block of 12 rows (0 to 11, 12 to 23, ...) at most 5 rows name the same one
- route_weights: float32 [192, 6], P('ep'), may hold values from 0.05 to 1
- expert_gate: bfloat16 [16, 4096, 1024], P('ep', 'tp'), may hold values from -0.09375 to 0.09375
- expert_up: bfloat16 [16, 4096, 1024], P('ep', 'tp'), may hold values from -0.09375 to 0.09375
- expert_down: bfloat16 [16, 1024, 4096], P('ep', None, 'tp'), may hold values from -0.1875 to 0.1875
- shared_gate: bfloat16 [4096, 1024], P('tp'), may hold values from -0.09375 to 0.09375
- shared_up: bfloat16 [4096, 1024], P('tp'), may hold values from -0.09375 to 0.09375
- shared_down: bfloat16 [1024, 4096], P(None, 'tp'), may hold values from -0.1875 to 0.1875
Outputs:
- mixed: bfloat16 [192, 4096], P('ep', 'tp')
The draws below stay inside these ranges and needn't reach their ends.
Inputs may be any that keep to these rules, and one draw needn't show every extreme that they name: `routes`: each row names 6 different experts; among the rows of one device no expert is named more than 5 times, and in some devices' rows one expert is named exactly 5 times.
All inputs are finite; a program needn't handle non-finite values.
Results may differ from the reference program's by a relative error of at most 0.0068.
Values may be sent and summed in bfloat16 or wider, within the bound.
No kernel may reach another device: no remote copies, remote signals or barrier semaphores. Data moves between devices by JAX's collectives and lax.ppermute only.
A program may use at most 64 MiB of HBM per device.

```python
import math
import jax
import jax.numpy as jnp
import numpy as np
from jax import lax

D = 4096
FF_E = 1024
FF_S = 1024
TOP_K = 6
TOK_DEV = 12
EXPERTS = 16
CAP = 5
TOKENS = 192
N_EP = 16


def draw_tokens(key, part):
    first, second = jax.random.split(jax.random.fold_in(key, 11), 2)
    column = jnp.arange(D, dtype=jnp.float32) / D
    rising = jnp.exp(jnp.log(8.0) * column)[None, :]
    base = jax.random.normal(first, (TOKENS, D), jnp.float32)
    rough = jax.random.uniform(second, (1, D), jnp.float32, 0.5, 1.5)
    values = jnp.clip(base, -6.0, 6.0) * rough * rising
    return values.astype(jnp.bfloat16)


def block_levels(key, shape, cuts, least, high):
    def one(dim, parts):
        steps = jax.random.uniform(jax.random.fold_in(jax.random.fold_in(key, 6), dim), (parts,), jnp.float32, least / len(cuts), high / len(cuts))
        return jnp.repeat(jnp.exp(steps), shape[dim] // parts).reshape((-1,) + (1,) * (len(shape) - dim - 1))

    level = one(*cuts[0])
    for cut in cuts[1:]:
        level = level * one(*cut)
    return level


def deal_out(stream_key, own, number, rows, count, top, limit, lean):
    sequence = jax.random.permutation(stream_key, count)
    heavy_load, common = shares(count, rows * top, limit, lean, True), shares(count, rows * top, limit, lean, False)
    places = jnp.arange(count)

    def named(tallies, offset_by):
        used = int((tallies > 0).sum())
        fixed = max(1, used // 4)
        moved = fixed + (places - fixed + offset_by * (used - fixed)) % max(1, count - fixed)
        return jnp.zeros((count,), jnp.int32).at[sequence[jnp.where(places < fixed, places, moved)]].set(jnp.asarray(tallies, jnp.int32))

    tallies = jnp.where(number % 4 == 0, named(heavy_load, number // 4), named(common, number - number // 4 - 1))
    mixed = jax.random.permutation(jax.random.fold_in(own, 3), count)
    donor, receiver = mixed[0:count // 2 * 2:2], mixed[1:count // 2 * 2:2]
    room = jnp.minimum(tallies[donor] - 1, limit - tallies[receiver]) // 2
    room = jnp.where((donor == sequence[0]) | (receiver == sequence[0]) | (tallies[receiver] == 0), 0, jnp.maximum(room, 0))
    moved = jax.random.randint(jax.random.fold_in(own, 4), (count // 2,), 0, 1 << 20) % (room + 1)
    tallies = tallies.at[donor].add(-moved).at[receiver].add(moved)
    labels = jnp.searchsorted(jnp.cumsum(tallies), jnp.arange(rows * top), side="right").astype(jnp.int32)
    grid = labels.reshape(top, rows).T
    grid = grid[jax.random.permutation(jax.random.fold_in(own, 1), rows)]
    offset_by = jax.random.randint(jax.random.fold_in(own, 2), (rows, 1), 0, top)
    return jnp.take_along_axis(grid, (jnp.arange(top)[None, :] + offset_by) % top, axis=1)


def shares(count, total, most, slope, full):
    weights = [(1 << 20) // math.isqrt(rank ** slope) + 1 for rank in range(1, count + 1)]
    largest = most if full else min(most, max(-(-total // count), total * weights[0] // sum(weights)))
    least = 1 if total - largest >= count - 1 else 0
    given, spare = [largest] + [least] * (count - 1), total - largest - least * (count - 1)
    while spare > 0:
        free = [i for i in range(1, count) if given[i] < largest] or [i for i in range(1, count) if given[i] < most]
        whole, budget = sum([weights[i] for i in free]), spare
        for i in free:
            addition = min(most - given[i], max(1, budget * weights[i] // whole), spare)
            given[i] = given[i] + addition
            spare = spare - addition
    return np.array(given)


def normal_values(own_key, dims, width, bound, cuts=(), held_as=jnp.bfloat16):
    entries = jax.random.normal(own_key, dims, jnp.float32) * width
    if len(cuts) > 0:
        entries = block_levels(own_key, dims, cuts, -0.22, 0.18) * entries
    return jnp.clip(entries, min=-bound, max=bound).astype(held_as)


def setup_inputs(seed: int = 0) -> dict:
    streams_of = jax.random.split(jax.random.key(seed), 11)
    tokens = draw_tokens(jax.random.fold_in(streams_of[10], 71), 0)
    norm_gain = jnp.clip(1.0 + 0.18 * jax.random.normal(streams_of[1], (D,), jnp.float32), 0.1, 1.9)
    routes_keys = jax.random.split(jax.random.fold_in(streams_of[2], 1), TOKENS // TOK_DEV)
    routes_turns = jax.random.permutation(jax.random.fold_in(streams_of[2], 3), TOKENS // TOK_DEV)
    routes = jax.vmap(lambda own, number: deal_out(jax.random.fold_in(streams_of[2], 2), own, number, TOK_DEV, EXPERTS, TOP_K, CAP, 2))(routes_keys, routes_turns).reshape((TOKENS, TOP_K))
    route_weights = jnp.clip(jnp.exp(math.log(1.0) - 2.9957323 * jax.random.uniform(streams_of[3], (TOKENS, TOP_K), jnp.float32) ** block_levels(streams_of[3], (TOKENS, TOP_K), ((0, 16),), -0.2, 0.2)), 0.05, 1.0)
    expert_gate = normal_values(streams_of[4], (EXPERTS, D, FF_E), D ** -0.5, 0.09375, ((0, 16), (1, 2)))
    expert_up = normal_values(streams_of[5], (EXPERTS, D, FF_E), D ** -0.5, 0.09375, ((0, 16), (1, 2)))
    expert_down = normal_values(streams_of[6], (EXPERTS, FF_E, D), FF_E ** -0.5, 0.1875, ((0, 16), (2, 2)))
    shared_gate = normal_values(streams_of[7], (D, FF_S), D ** -0.5, 0.09375, ((0, 2),))
    shared_up = normal_values(streams_of[8], (D, FF_S), D ** -0.5, 0.09375, ((0, 2),))
    shared_down = normal_values(streams_of[9], (FF_S, D), FF_S ** -0.5, 0.1875, ((1, 2),))
    return {"tokens": tokens, "norm_gain": norm_gain, "routes": routes, "route_weights": route_weights, "expert_gate": expert_gate, "expert_up": expert_up, "expert_down": expert_down, "shared_gate": shared_gate, "shared_up": shared_up, "shared_down": shared_down}


def block_ranks(route_blocks, n_experts):
    onehot = (route_blocks[..., None] == jnp.arange(n_experts, dtype=jnp.int32)).astype(jnp.int32)
    before = jnp.cumsum(onehot, axis=1) - onehot
    return lax.optimization_barrier(jnp.sum(before * onehot, axis=-1))

def expert_tables(route_blocks, weight_blocks, expert, capacity, n_experts):
    blocks, tok, picks = route_blocks.shape
    ranks = block_ranks(route_blocks.reshape(blocks, tok * picks), n_experts).reshape(blocks, tok, picks)
    slot = jnp.where(route_blocks == expert, ranks, -1)
    hits = slot[..., None] == jnp.arange(capacity, dtype=jnp.int32)
    select = jnp.any(hits, axis=2).astype(jnp.float32)
    weighted = lax.optimization_barrier(jnp.sum(jnp.where(hits, weight_blocks[..., None], 0.0), axis=2))
    return (select, weighted)

def swiglu(rows, gate_w, up_w, down_w):
    gate = jnp.dot(rows, gate_w, preferred_element_type=jnp.float32)
    up = jnp.dot(rows, up_w, preferred_element_type=jnp.float32)
    hidden = (jax.nn.silu(gate) * up).astype(jnp.bfloat16)
    return jnp.dot(hidden, down_w, preferred_element_type=jnp.float32)

def reference(tokens, norm_gain, routes, route_weights, expert_gate, expert_up, expert_down, shared_gate, shared_up, shared_down):
    values = tokens.astype(jnp.float32)
    meansq = lax.optimization_barrier(jnp.mean(values * values, axis=1, keepdims=True))
    normed = (values * lax.rsqrt(meansq + 1e-06) * norm_gain.astype(jnp.float32)[None, :]).astype(jnp.bfloat16)
    scaled = 2.5 * route_weights / lax.optimization_barrier(jnp.sum(route_weights, axis=1, keepdims=True))
    shared_out = swiglu(normed, shared_gate, shared_up, shared_down)
    capacity = max(2, TOK_DEV * TOP_K // N_EP + 1)
    route_blocks = routes.reshape(N_EP, TOK_DEV, TOP_K)
    weight_blocks = scaled.reshape(N_EP, TOK_DEV, TOP_K)
    x_blocks = normed.reshape(N_EP, TOK_DEV, D).astype(jnp.float32)

    def one_expert(carry, packed):
        gate_w, up_w, down_w, expert = packed
        select, weighted = expert_tables(route_blocks, weight_blocks, expert, capacity, EXPERTS)
        rows = jnp.einsum('stc,std->scd', select, x_blocks).astype(jnp.bfloat16)
        result = swiglu(rows.reshape(N_EP * capacity, D), gate_w, up_w, down_w).astype(jnp.bfloat16)
        result = result.reshape(N_EP, capacity, D).astype(jnp.float32)
        carry = carry + jnp.einsum('stc,scd->std', weighted, result, precision=lax.Precision.HIGHEST)
        return (carry, None)
    start = jnp.zeros((N_EP, TOK_DEV, D), jnp.float32)
    routed, _ = lax.scan(one_expert, start, (expert_gate, expert_up, expert_down, jnp.arange(EXPERTS, dtype=jnp.int32)))
    return (shared_out + routed.reshape(TOKENS, D)).astype(jnp.bfloat16)
```

```python
import functools

import jax
import jax.numpy as jnp
from jax import lax
from jax.experimental import pallas as pl
from jax.experimental.pallas import tpu as pltpu
from jax.sharding import PartitionSpec as P

F32 = jnp.float32
BF16 = jnp.bfloat16
LANES = 128
VMEM = pl.BlockSpec(memory_space=pltpu.VMEM)


def call(body, name, outs, n_in, scratch=(), flops=0, limit=16):
    return pl.pallas_call(
        body,
        name=name,
        out_shape=outs,
        in_specs=[VMEM] * n_in,
        out_specs=jax.tree.map(lambda _: VMEM, outs),
        scratch_shapes=list(scratch),
        cost_estimate=pl.CostEstimate(flops=flops, bytes_accessed=0, transcendentals=0),
        compiler_params=pltpu.CompilerParams(vmem_limit_bytes=limit * 2**20),
    )


def resident(weight):
    return pltpu.with_memory_space_constraint(weight, pltpu.VMEM)


def dispatch_body(cap, split, tok_ref, routes_ref, weight_ref, out_ref, comb_ref, wide):
    tok, width = tok_ref.shape
    picks = routes_ref.shape[1]
    slots = comb_ref.shape[1]
    part = width // split
    routes = routes_ref[...]
    weights = weight_ref[...]
    scaled = 2.5 * weights / jnp.sum(weights, axis=1, keepdims=True)
    slot = lax.broadcasted_iota(jnp.int32, (tok, slots), 1)
    expert_f = jnp.floor((slot.astype(F32) + 0.5) * (1.0 / cap))
    expert = expert_f.astype(jnp.int32)
    rank = (slot - expert * cap).astype(F32)
    named = jnp.zeros((tok, slots), F32)
    gain = jnp.zeros((tok, slots), F32)
    for k in range(picks):
        same = routes[:, k : k + 1] == expert
        named = jnp.where(same, 1.0, named)
        gain = jnp.where(same, scaled[:, k : k + 1], gain)
    row = lax.broadcasted_iota(jnp.int32, (tok, tok), 0)
    col = lax.broadcasted_iota(jnp.int32, (tok, tok), 1)
    earlier = jnp.where(col < row, 1.0, 0.0).astype(BF16)
    before = jnp.dot(earlier, named.astype(BF16), preferred_element_type=F32)
    hit = jnp.where(before == rank, named, 0.0)
    comb_ref[...] = hit * gain
    pick = hit.astype(BF16)
    step = 2 * part
    for q in range(0, split, 2):
        rows = lax.dot_general(
            pick,
            tok_ref[:, q * part : q * part + step],
            (((0,), (0,)), ((), ())),
            preferred_element_type=F32,
        )
        wide[pl.ds(q, slots, stride=split), :] = rows[:, :part]
        wide[pl.ds(q + 1, slots, stride=split), :] = rows[:, part:]
    out_ref[...] = wide[...].astype(BF16)


def shared_in_body(tok_ref, gain_ref, gate_ref, up_ref, part_ref, sq_ref):
    hidden = gate_ref.shape[1]
    values = tok_ref[...].astype(F32)
    sq_ref[...] = jnp.broadcast_to(jnp.sum(values * values, axis=1, keepdims=True), sq_ref.shape)
    rows = (values * gain_ref[...]).astype(BF16)
    part_ref[:, :hidden] = jnp.dot(rows, gate_ref[...], preferred_element_type=F32)
    part_ref[:, hidden:] = jnp.dot(rows, up_ref[...], preferred_element_type=F32)


def squares_tail(total):
    lane = lax.broadcasted_iota(jnp.int32, (total.shape[0], LANES), 1)
    high = total.astype(BF16).astype(F32)
    return jnp.where(lane == 0, high, jnp.where(lane == 1, total - high, 0.0))


def expert_in_body(
    split, rows_ref, gain_ref, gate_ref, up_ref, part_ref, sq_ref, send_ref, keep_ref, wide, lhs
):
    hidden = gate_ref.shape[1]
    slots = lhs.shape[0]
    tok = part_ref.shape[0]
    part = rows_ref.shape[1]
    wide[...] = rows_ref[...].astype(F32)
    squares = jnp.zeros((slots, part), F32)
    for q in range(split):
        values = wide[pl.ds(q, slots, stride=split), :]
        squares = squares + values * values
        gain = gain_ref[:, q * part : (q + 1) * part]
        lhs[:, q * part : (q + 1) * part] = (values * gain).astype(BF16)
    keep_ref[slots:, :] = jnp.zeros((keep_ref.shape[0] - slots, keep_ref.shape[1]), F32)
    keep_ref[slots : slots + tok, : 2 * hidden] = part_ref[...]
    keep_ref[slots : slots + tok, 2 * hidden :] = squares_tail(sq_ref[:, :1])
    keep_ref[:slots, 2 * hidden :] = squares_tail(jnp.sum(squares, axis=1, keepdims=True))
    keep_ref[:slots, :hidden] = jnp.dot(lhs[...], gate_ref[...], preferred_element_type=F32)
    keep_ref[:slots, hidden : 2 * hidden] = jnp.dot(
        lhs[...], up_ref[...], preferred_element_type=F32
    )
    send_ref[...] = keep_ref[...].astype(BF16)


def expert_out_body(split, width, n_recv, *refs):
    keep_ref, recv_refs, down_ref = refs[0], refs[1 : 1 + n_recv], refs[1 + n_recv]
    out_ref, shared_ref, wide = refs[2 + n_recv :]
    hidden, cols = down_ref.shape
    slots = out_ref.shape[0] // split
    part = cols // split
    total = keep_ref[...]
    for recv in recv_refs:
        total = total + recv[...].astype(F32)
    squares = jnp.sum(total[:, 2 * hidden :], axis=1, keepdims=True)
    scale = lax.rsqrt(squares / width + 1e-06)
    gate = total[:, :hidden] * scale
    up = total[:, hidden : 2 * hidden] * scale
    act = (gate / (1.0 + jnp.exp(-gate)) * up).astype(BF16)
    shared_ref[...] = act[slots:]
    step = 2 * part
    for q in range(0, split, 2):
        rows = jnp.dot(
            act[:slots], down_ref[:, q * part : q * part + step], preferred_element_type=F32
        )
        wide[pl.ds(q, slots, stride=split), :] = rows[:, :part]
        wide[pl.ds(q + 1, slots, stride=split), :] = rows[:, part:]
    out_ref[...] = wide[...].astype(BF16)


def shared_out_body(hidden_ref, down_ref, out_ref):
    tok = out_ref.shape[0]
    out_ref[...] = jnp.dot(hidden_ref[...], down_ref[...], preferred_element_type=F32)[:tok]


def combine_body(split, back_ref, comb_ref, shared_ref, out_ref, wide):
    slots = comb_ref.shape[1]
    part = back_ref.shape[1]
    wide[...] = back_ref[...].astype(F32)
    comb = comb_ref[...]
    high = comb.astype(BF16)
    rest = comb - high.astype(F32)
    mid = rest.astype(BF16)
    low = (rest - mid.astype(F32)).astype(BF16)
    for q in range(split):
        values = wide[pl.ds(q, slots, stride=split), :].astype(BF16)
        total = shared_ref[:, q * part : (q + 1) * part]
        for piece in (low, mid, high):
            total = total + jnp.dot(piece, values, preferred_element_type=F32)
        out_ref[:, q * part : (q + 1) * part] = total.astype(BF16)


def local(
    tokens,
    norm_gain,
    routes,
    route_weights,
    expert_gate,
    expert_up,
    expert_down,
    shared_gate,
    shared_up,
    shared_down,
):
    tok, width = tokens.shape
    picks = routes.shape[1]
    n_tp, n_ep = lax.axis_size("tp"), lax.axis_size("ep")
    cap = max(2, tok * picks // n_ep + 1)
    slots = n_ep * cap
    split = width // LANES
    part = LANES
    hidden = expert_gate.shape[2]
    rows = slots + -(-tok // 16) * 16
    cols = 2 * hidden + LANES
    sds = jax.ShapeDtypeStruct
    gain = norm_gain.reshape(1, width)
    gate_w, up_w, down_w = expert_gate[0], expert_up[0], expert_down[0]

    outgoing, comb = call(
        functools.partial(dispatch_body, cap, split),
        "dispatch",
        (sds((slots * split, part), BF16), sds((tok, slots), F32)),
        3,
        [pltpu.VMEM((slots * split, part), F32)],
        2 * tok * slots * width,
    )(tokens, routes, route_weights)
    arrived = lax.all_to_all(
        outgoing.reshape(n_ep, cap * split, part), "ep", split_axis=0, concat_axis=0, tiled=True
    ).reshape(slots * split, part)
    shared_part, shared_sq = call(
        shared_in_body,
        "shared_in",
        (sds((tok, 2 * hidden), F32), sds((tok, LANES), F32)),
        4,
        (),
        4 * 128 * width * hidden,
    )(tokens, gain, resident(shared_gate), resident(shared_up))
    send, keep = call(
        functools.partial(expert_in_body, split),
        "expert_in",
        (sds((rows, cols), BF16), sds((rows, cols), F32)),
        6,
        [pltpu.VMEM((slots * split, part), F32), pltpu.VMEM((slots, width), BF16)],
        4 * slots * width * hidden,
    )(arrived, gain, resident(gate_w), resident(up_w), shared_part, shared_sq)
    received = [
        lax.ppermute(send, "tp", [(i, (i + s) % n_tp) for i in range(n_tp)])
        for s in range(1, n_tp)
    ]
    result, shared_hidden = call(
        functools.partial(expert_out_body, split, width * n_tp, n_tp - 1),
        "expert_out",
        (sds((slots * split, part), BF16), sds((rows - slots, hidden), BF16)),
        n_tp + 1,
        [pltpu.VMEM((slots * split, part), F32)],
        2 * slots * width * hidden,
    )(keep, *received, resident(down_w))
    back = lax.all_to_all(
        result.reshape(n_ep, cap * split, part), "ep", split_axis=0, concat_axis=0, tiled=True
    ).reshape(slots * split, part)
    shared_out = call(
        shared_out_body, "shared_out", sds((tok, width), F32), 2, (), 2 * 128 * width * hidden
    )(shared_hidden, resident(shared_down))
    return call(
        functools.partial(combine_body, split),
        "combine",
        sds((tok, width), BF16),
        3,
        [pltpu.VMEM((slots * split, part), F32)],
        6 * tok * slots * width,
    )(back, comb, shared_out)


def solution(mesh):
    placed = (
        P("ep", "tp"),
        P("tp"),
        P("ep", None),
        P("ep", None),
        P("ep", "tp", None),
        P("ep", "tp", None),
        P("ep", None, "tp"),
        P("tp", None),
        P("tp", None),
        P(None, "tp"),
    )
    return jax.shard_map(
        local, mesh=mesh, in_specs=placed, out_specs=P("ep", "tp"), check_vma=False
    )
```

```python
import functools

import jax
import jax.numpy as jnp
from jax import lax
from jax.experimental import pallas as pl
from jax.experimental.pallas import tpu as pltpu
from jax.sharding import PartitionSpec as P

F32 = jnp.float32
BF16 = jnp.bfloat16
LANES = 128
VMEM = pl.BlockSpec(memory_space=pltpu.VMEM)
HBM = pl.BlockSpec(memory_space=pltpu.HBM)


def call(body, name, outs, ins, scratch=(), flops=0, limit=16):
    return pl.pallas_call(
        body,
        name=name,
        out_shape=outs,
        in_specs=list(ins),
        out_specs=jax.tree.map(lambda _: VMEM, outs),
        scratch_shapes=list(scratch),
        cost_estimate=pl.CostEstimate(flops=flops, bytes_accessed=0, transcendentals=0),
        compiler_params=pltpu.CompilerParams(vmem_limit_bytes=limit * 2**20),
    )


def stored(value):
    return pltpu.with_memory_space_constraint(value, pltpu.HBM)


def start_copies(pairs, sems):
    copies = [pltpu.make_async_copy(src, dst, sems.at[i]) for i, (src, dst) in enumerate(pairs)]
    for copy in copies:
        copy.start()
    return copies


def dot(a, b):
    return jnp.dot(a, b, preferred_element_type=F32)


def shard(size, index):
    return pl.ds(pl.multiple_of(index * size, size), size)


def peer(step):
    return lax.rem(lax.axis_index("tp") + step, lax.axis_size("tp"))


def dispatch_body(cap, tok_hbm, routes_hbm, weight_hbm, out_ref, comb_ref, *scratch):
    wide, tok_ref, routes_ref, weight_ref, sems = scratch
    copies = start_copies(
        ((routes_hbm, routes_ref), (weight_hbm, weight_ref), (tok_hbm, tok_ref)), sems
    )
    tok, width = tok_ref.shape
    picks = routes_ref.shape[0]
    slots = comb_ref.shape[1]
    split = width // LANES
    slot = lax.broadcasted_iota(jnp.int32, (slots, tok), 0)
    expert = jnp.floor((slot.astype(F32) + 0.5) * (1.0 / cap)).astype(jnp.int32)
    rank = (slot - expert * cap).astype(F32)
    row = lax.broadcasted_iota(jnp.int32, (tok, tok), 0)
    col = lax.broadcasted_iota(jnp.int32, (tok, tok), 1)
    earlier = jnp.where(row < col, 1.0, 0.0).astype(BF16)
    copies[0].wait()
    copies[1].wait()
    routes = routes_ref[...]
    weights = weight_ref[...]
    scaled = 2.5 * weights / jnp.sum(weights, axis=0, keepdims=True)
    named = jnp.zeros((slots, tok), F32)
    gain = jnp.zeros((slots, tok), F32)
    for k in range(picks):
        same = routes[k : k + 1, :] == expert
        named = jnp.where(same, 1.0, named)
        gain = jnp.where(same, scaled[k : k + 1, :], gain)
    before = dot(named.astype(BF16), earlier)
    hit = jnp.where(before == rank, named, 0.0)
    pick = hit.astype(BF16)
    copies[2].wait()
    for q in range(0, split, 2):
        rows = dot(pick, tok_ref[:, q * LANES : (q + 2) * LANES])
        wide[pl.ds(q, slots, stride=split), :] = rows[:, :LANES]
        wide[pl.ds(q + 1, slots, stride=split), :] = rows[:, LANES:]
    out_ref[...] = wide[...].astype(BF16)
    comb_ref[...] = jnp.transpose(hit * gain)


def squares_tail(total):
    lane = lax.broadcasted_iota(jnp.int32, (total.shape[0], LANES), 1)
    high = total.astype(BF16).astype(F32)
    return jnp.where(lane == 0, high, jnp.where(lane == 1, total - high, 0.0))


def window_body(tok_hbm, gain_hbm, gate_hbm, up_hbm, first_hbm, *refs):
    keep_ref, send_ref, gain_ref, first_ref, tok_ref, gate_ref, up_ref, sems = refs
    pairs = ((tok_hbm, tok_ref), (gain_hbm, gain_ref), (gate_hbm, gate_ref), (up_hbm, up_ref))
    first = first_hbm.at[:, shard(first_ref.shape[1], peer(1))]
    copies = start_copies(pairs + ((first, first_ref),), sems)
    hidden = gate_ref.shape[1]
    tok = tok_ref.shape[0]
    keep_ref[...] = jnp.zeros_like(keep_ref)
    copies[0].wait()
    copies[1].wait()
    values = tok_ref[...].astype(F32)
    keep_ref[:tok, 2 * hidden :] = squares_tail(jnp.sum(values * values, axis=1, keepdims=True))
    rows = (values * gain_ref[...]).astype(BF16)
    copies[2].wait()
    keep_ref[:tok, :hidden] = dot(rows, gate_ref[...])
    copies[3].wait()
    keep_ref[:tok, hidden : 2 * hidden] = dot(rows, up_ref[...])
    send_ref[...] = keep_ref[...].astype(BF16)
    copies[4].wait()


def hidden_units(total, hidden, width):
    squares = jnp.sum(total[:, 2 * hidden :], axis=1, keepdims=True)
    scale = lax.rsqrt(squares / width + 1e-06)
    gate = total[:, :hidden] * scale
    up = total[:, hidden : 2 * hidden] * scale
    return (gate / (1.0 + jnp.exp(-gate)) * up).astype(BF16)


def shared_out_body(width, keep_ref, *refs):
    recv_refs, down_hbm, out_ref, buf, sems = refs[:-4], *refs[-4:]
    step = buf.shape[2]
    copies = start_copies(
        [(down_hbm.at[:, i * step : (i + 1) * step], buf.at[i]) for i in range(buf.shape[0])],
        sems,
    )
    total = keep_ref[...]
    for recv in recv_refs:
        total = total + recv[...].astype(F32)
    act = hidden_units(total, buf.shape[1], width)
    for i, copy in enumerate(copies):
        copy.wait()
        out_ref[:, i * step : (i + 1) * step] = dot(act, buf[i])[: out_ref.shape[0]]


def column_copies(weights, owner, size, buf, base):
    step = buf.shape[2]
    pairs = []
    for weight in weights:
        for i in range(size // step):
            cols = pl.ds(pl.multiple_of(owner * size + i * step, step), step)
            pairs.append((weight.at[:, cols], buf.at[base + len(pairs)]))
    return pairs


def expert_send_body(n_send, rows_ref, gain_ref, first_ref, gate_hbm, up_hbm, *refs):
    send_refs, (lhs_ref, tail_ref, wide, buf, sems) = refs[:n_send], refs[n_send:]
    slots, width = lhs_ref.shape
    split = width // LANES
    size, step = first_ref.shape[1], buf.shape[2]
    pairs = []
    for k in range(1, n_send + 1):
        weights = (up_hbm,) if k == 1 else (gate_hbm, up_hbm)
        pairs += column_copies(weights, peer(k), size, buf, len(pairs))
    copies = start_copies(pairs, sems)
    wide[...] = rows_ref[...].astype(F32)
    squares = jnp.zeros((slots, LANES), F32)
    for q in range(split):
        values = wide[pl.ds(q, slots, stride=split), :]
        squares = squares + values * values
        cols = slice(q * LANES, (q + 1) * LANES)
        lhs_ref[:, cols] = (values * gain_ref[:, cols]).astype(BF16)
    tail = squares_tail(jnp.sum(squares, axis=1, keepdims=True))
    tail_ref[...] = tail
    done = 0
    for k, send in enumerate(send_refs, 1):
        send[:, 2 * size :] = tail.astype(BF16)
        if k == 1:
            send[:, :size] = dot(lhs_ref[...], first_ref[...]).astype(BF16)
        for i in range(size if k == 1 else 0, 2 * size, step):
            copies[done].wait()
            send[:, i : i + step] = dot(lhs_ref[...], buf[done]).astype(BF16)
            done += 1


def expert_keep_body(lhs_ref, tail_ref, gate_hbm, up_hbm, keep_ref, buf, sems):
    size, step = (keep_ref.shape[1] - LANES) // 2, buf.shape[2]
    copies = start_copies(column_copies((gate_hbm, up_hbm), peer(0), size, buf, 0), sems)
    keep_ref[:, 2 * size :] = tail_ref[...]
    for i, copy in enumerate(copies):
        copy.wait()
        keep_ref[:, i * step : (i + 1) * step] = dot(lhs_ref[...], buf[i])


def expert_mid_body(width, keep_ref, *refs):
    recv_refs, out_ref = refs[:-1], refs[-1]
    total = keep_ref[...]
    for recv in recv_refs:
        total = total + recv[...].astype(F32)
    out_ref[...] = hidden_units(total, out_ref.shape[1], width)


def down_keep_body(act_ref, down_ref, acc_ref):
    acc_ref[...] = dot(act_ref[...], down_ref[shard(act_ref.shape[1], peer(0)), :])


def down_rest_body(acc_ref, down_ref, *refs):
    recv_refs, out_ref, wide = refs[:-2], refs[-2], refs[-1]
    slots, width = acc_ref.shape
    split = width // LANES
    n_tp = len(recv_refs) + 1
    for q in range(0, split, 2):
        cols = slice(q * LANES, (q + 2) * LANES)
        rows = acc_ref[:, cols]
        for step, recv in enumerate(recv_refs, 1):
            owner = shard(recv.shape[1], peer(n_tp - step))
            rows = rows + dot(recv[...], down_ref[owner, cols])
        wide[pl.ds(q, slots, stride=split), :] = rows[:, :LANES]
        wide[pl.ds(q + 1, slots, stride=split), :] = rows[:, LANES:]
    out_ref[...] = wide[...].astype(BF16)


def combine_body(back_ref, comb_ref, shared_ref, out_ref, wide):
    tok, width = out_ref.shape
    slots = comb_ref.shape[1]
    split = width // LANES
    wide[...] = back_ref[...].astype(F32)
    comb = comb_ref[...]
    high = comb.astype(BF16)
    rest = comb - high.astype(F32)
    mid = rest.astype(BF16)
    for q in range(0, split, 2):
        cols = slice(q * LANES, (q + 2) * LANES)
        values = jnp.concatenate(
            [
                wide[pl.ds(q, slots, stride=split), :].astype(BF16),
                wide[pl.ds(q + 1, slots, stride=split), :].astype(BF16),
            ],
            axis=1,
        )
        total = shared_ref[:, cols] + dot(mid, values) + dot(high, values)
        out_ref[:, cols] = total.astype(BF16)


def shift(value, step):
    size = lax.axis_size("tp")
    return lax.ppermute(value, "tp", [(i, (i + step) % size) for i in range(size)])


def experts_plain(arrived, gain, gate_w, up_w, down_w, slots, width):
    values = arrived.reshape(slots, width).astype(F32)
    total = lax.psum(jnp.sum(values * values, axis=1, keepdims=True), "tp")
    normed = values * lax.rsqrt(total / (width * lax.axis_size("tp")) + 1e-06) * gain
    rows = normed.astype(BF16)
    gate, up = (
        lax.psum_scatter(dot(rows, w), "tp", scatter_dimension=1, tiled=True)
        for w in (gate_w, up_w)
    )
    act = lax.all_gather((jax.nn.silu(gate) * up).astype(BF16), "tp", axis=1, tiled=True)
    return dot(act, down_w).astype(BF16).reshape(arrived.shape)


def experts(arrived, gain, first, gate_w, up_w, down_w, slots, width):
    n_tp = lax.axis_size("tp")
    hidden = gate_w.shape[1]
    size = hidden // n_tp
    if size % LANES != 0:
        return experts_plain(arrived, gain, gate_w, up_w, down_w, slots, width)
    sds = jax.ShapeDtypeStruct
    work = 4 * slots * width * size
    step = 2 * LANES if size % (2 * LANES) == 0 else LANES
    pieces = size // step

    def streamed(count):
        return [pltpu.VMEM((count, width, step), BF16), pltpu.SemaphoreType.DMA((count,))]

    *sends, lhs, tail = call(
        functools.partial(expert_send_body, n_tp - 1),
        "expert_send",
        tuple(sds((slots, 2 * size + LANES), BF16) for _ in range(n_tp - 1))
        + (sds((slots, width), BF16), sds((slots, LANES), F32)),
        [VMEM] * 3 + [HBM] * 2,
        [pltpu.VMEM(arrived.shape, F32)] + streamed(pieces * (2 * n_tp - 3)),
        work * (n_tp - 1),
    )(arrived, gain, first, stored(gate_w), stored(up_w))
    received = [shift(send, step) for step, send in enumerate(sends, 1)]
    keep = call(
        expert_keep_body,
        "expert_keep",
        sds((slots, 2 * size + LANES), F32),
        [VMEM] * 2 + [HBM] * 2,
        streamed(pieces * 2),
        work,
    )(lhs, tail, stored(gate_w), stored(up_w))
    act = call(
        functools.partial(expert_mid_body, width * n_tp),
        "expert_mid",
        sds((slots, size), BF16),
        [VMEM] * n_tp,
        (),
        10 * slots * size,
    )(keep, *received)
    acts = [shift(act, step) for step in range(1, n_tp)]
    acc = call(
        down_keep_body, "down_keep", sds((slots, width), F32), [VMEM] * 2, (), work // 2
    )(act, down_w)
    return call(
        down_rest_body,
        "down_rest",
        pltpu.VMEM(arrived.shape, BF16),
        [VMEM] * (n_tp + 1),
        [pltpu.VMEM(arrived.shape, F32)],
        work // 2 * (n_tp - 1),
    )(acc, down_w, *acts)


def local(
    tokens,
    norm_gain,
    routes,
    route_weights,
    expert_gate,
    expert_up,
    expert_down,
    shared_gate,
    shared_up,
    shared_down,
):
    tok, width = tokens.shape
    picks = routes.shape[1]
    n_tp, n_ep = lax.axis_size("tp"), lax.axis_size("ep")
    cap = max(2, tok * picks // n_ep + 1)
    slots = n_ep * cap
    split = width // LANES
    hidden = expert_gate.shape[2]
    tok_rows = -(-tok // 16) * 16
    cols = 2 * hidden + LANES
    sds = jax.ShapeDtypeStruct
    sem = pltpu.SemaphoreType.DMA

    def exchange(value):
        blocks = value.reshape(n_ep, cap * split, LANES)
        moved = lax.all_to_all(blocks, "ep", split_axis=0, concat_axis=0, tiled=True)
        return moved.reshape(slots * split, LANES)

    outgoing, comb = call(
        functools.partial(dispatch_body, cap),
        "dispatch",
        (pltpu.VMEM((slots * split, LANES), BF16), sds((tok, slots), F32)),
        [HBM] * 3,
        [
            pltpu.VMEM((slots * split, LANES), F32),
            pltpu.VMEM((tok, width), BF16),
            pltpu.VMEM((picks, tok), jnp.int32),
            pltpu.VMEM((picks, tok), F32),
            sem((3,)),
        ],
        2 * tok * slots * width,
    )(*map(stored, (tokens, routes.T, route_weights.T)))
    arrived = exchange(outgoing)
    gate_w, up_w, down_w = expert_gate[0], expert_up[0], expert_down[0]
    size = hidden // n_tp if hidden % (n_tp * LANES) == 0 else LANES
    shared_keep, shared_send, gain, first = call(
        window_body,
        "window",
        (sds((tok_rows, cols), F32), sds((tok_rows, cols), BF16), sds((1, width), F32))
        + (sds((width, size), BF16),),
        [HBM] * 5,
        [
            pltpu.VMEM((tok, width), BF16),
            pltpu.VMEM(shared_gate.shape, BF16),
            pltpu.VMEM(shared_up.shape, BF16),
            sem((5,)),
        ],
        4 * 256 * width * hidden,
    )(*map(stored, (tokens, norm_gain.reshape(1, width), shared_gate, shared_up, gate_w)))
    shared_received = [shift(shared_send, step) for step in range(1, n_tp)]
    result = experts(arrived, gain, first, gate_w, up_w, down_w, slots, width)
    back = exchange(result)
    chunks = next(c for c in (4, 2, 1) if width % (c * LANES) == 0)
    shared_out = call(
        functools.partial(shared_out_body, width * n_tp),
        "shared_out",
        sds((tok, width), F32),
        [VMEM] * n_tp + [HBM],
        [pltpu.VMEM((chunks, hidden, width // chunks), BF16), sem((chunks,))],
        2 * 128 * width * hidden,
    )(shared_keep, *shared_received, stored(shared_down))
    return call(
        combine_body,
        "combine",
        sds((tok, width), BF16),
        [VMEM] * 3,
        [pltpu.VMEM((slots * split, LANES), F32)],
        6 * tok * slots * width,
    )(back, comb, shared_out)


def solution(mesh):
    placed = (
        P("ep", "tp"),
        P("tp"),
        P("ep", None),
        P("ep", None),
        P("ep", "tp", None),
        P("ep", "tp", None),
        P("ep", None, "tp"),
        P("tp", None),
        P("tp", None),
        P(None, "tp"),
    )
    return jax.shard_map(
        local, mesh=mesh, in_specs=placed, out_specs=P("ep", "tp"), check_vma=False
    )
```

```python
import functools

import jax
import jax.numpy as jnp
from jax import lax
from jax.experimental import pallas as pl
from jax.experimental.pallas import tpu as pltpu
from jax.sharding import PartitionSpec as P

F32 = jnp.float32
BF16 = jnp.bfloat16
LANES = 128
VMEM = pl.BlockSpec(memory_space=pltpu.VMEM)
HBM = pl.BlockSpec(memory_space=pltpu.HBM)


def call(body, name, outs, ins, scratch=(), flops=0, limit=16):
    return pl.pallas_call(
        body,
        name=name,
        out_shape=outs,
        in_specs=list(ins),
        out_specs=jax.tree.map(lambda _: VMEM, outs),
        scratch_shapes=list(scratch),
        cost_estimate=pl.CostEstimate(flops=flops, bytes_accessed=0, transcendentals=0),
        compiler_params=pltpu.CompilerParams(vmem_limit_bytes=limit * 2**20),
    )


def stored(value):
    return pltpu.with_memory_space_constraint(value, pltpu.HBM)


def start_copies(pairs, sems):
    copies = [pltpu.make_async_copy(src, dst, sems.at[i]) for i, (src, dst) in enumerate(pairs)]
    for copy in copies:
        copy.start()
    return copies


def dot(a, b):
    return jnp.dot(a, b, preferred_element_type=F32)


def shard(size, index):
    return pl.ds(pl.multiple_of(index * size, size), size)


def peer(step):
    return lax.rem(lax.axis_index("tp") + step, lax.axis_size("tp"))


def dispatch_body(cap, n_send, tok_hbm, routes_hbm, weight_hbm, *refs):
    n_big = 3 if n_send else 0
    big_hbm, out_ref, comb_ref = refs[:n_big], refs[n_big], refs[n_big + 1]
    big_refs = refs[n_big + 2 : 2 * n_big + 2]
    wide, tok_ref, routes_ref, weight_ref, sems = refs[2 * n_big + 2 :]
    pairs = [(routes_hbm, routes_ref), (weight_hbm, weight_ref), (tok_hbm, tok_ref)]
    if n_send:
        pairs.append((big_hbm[0], big_refs[0]))
        for src, dst in zip(big_hbm[1:], big_refs[1:]):
            for k in range(n_send):
                pairs.append((src.at[:, shard(dst.shape[2], peer(k + 1))], dst.at[k]))
    copies = start_copies(pairs, sems)
    tok, width = tok_ref.shape
    picks = routes_ref.shape[0]
    slots = comb_ref.shape[1]
    split = width // LANES
    slot = lax.broadcasted_iota(jnp.int32, (slots, tok), 0)
    expert = jnp.floor((slot.astype(F32) + 0.5) * (1.0 / cap)).astype(jnp.int32)
    rank = (slot - expert * cap).astype(F32)
    row = lax.broadcasted_iota(jnp.int32, (tok, tok), 0)
    col = lax.broadcasted_iota(jnp.int32, (tok, tok), 1)
    earlier = jnp.where(row < col, 1.0, 0.0).astype(BF16)
    copies[0].wait()
    copies[1].wait()
    routes = routes_ref[...]
    weights = weight_ref[...]
    scaled = 2.5 * weights / jnp.sum(weights, axis=0, keepdims=True)
    named = jnp.zeros((slots, tok), F32)
    gain = jnp.zeros((slots, tok), F32)
    for k in range(picks):
        same = routes[k : k + 1, :] == expert
        named = jnp.where(same, 1.0, named)
        gain = jnp.where(same, scaled[k : k + 1, :], gain)
    before = dot(named.astype(BF16), earlier)
    hit = jnp.where(before == rank, named, 0.0)
    pick = hit.astype(BF16)
    copies[2].wait()
    for q in range(0, split, 2):
        rows = dot(pick, tok_ref[:, q * LANES : (q + 2) * LANES])
        wide[pl.ds(q, slots, stride=split), :] = rows[:, :LANES]
        wide[pl.ds(q + 1, slots, stride=split), :] = rows[:, LANES:]
    out_ref[...] = wide[...].astype(BF16)
    comb_ref[...] = jnp.transpose(hit * gain)
    for copy in copies[3:]:
        copy.wait()


def squares_tail(total):
    lane = lax.broadcasted_iota(jnp.int32, (total.shape[0], LANES), 1)
    high = total.astype(BF16).astype(F32)
    return jnp.where(lane == 0, high, jnp.where(lane == 1, total - high, 0.0))


def shared_in_body(tok_hbm, gain_hbm, gate_hbm, up_hbm, down_hbm, *refs):
    keep_ref, send_ref, down_ref, tok_ref, gain_ref, gate_ref, up_ref, sems = refs
    pairs = ((tok_hbm, tok_ref), (gain_hbm, gain_ref), (gate_hbm, gate_ref), (up_hbm, up_ref))
    copies = start_copies(pairs + ((down_hbm, down_ref),), sems)
    hidden = gate_ref.shape[1]
    tok = tok_ref.shape[0]
    keep_ref[...] = jnp.zeros_like(keep_ref)
    copies[0].wait()
    copies[1].wait()
    values = tok_ref[...].astype(F32)
    keep_ref[:tok, 2 * hidden :] = squares_tail(jnp.sum(values * values, axis=1, keepdims=True))
    rows = (values * gain_ref[...]).astype(BF16)
    copies[2].wait()
    keep_ref[:tok, :hidden] = dot(rows, gate_ref[...])
    copies[3].wait()
    keep_ref[:tok, hidden : 2 * hidden] = dot(rows, up_ref[...])
    send_ref[...] = keep_ref[...].astype(BF16)
    copies[4].wait()


def hidden_units(total, hidden, width):
    squares = jnp.sum(total[:, 2 * hidden :], axis=1, keepdims=True)
    scale = lax.rsqrt(squares / width + 1e-06)
    gate = total[:, :hidden] * scale
    up = total[:, hidden : 2 * hidden] * scale
    return (gate / (1.0 + jnp.exp(-gate)) * up).astype(BF16)


def shared_out_body(width, keep_ref, *refs):
    recv_refs, down_ref, out_ref = refs[:-2], refs[-2], refs[-1]
    total = keep_ref[...]
    for recv in recv_refs:
        total = total + recv[...].astype(F32)
    act = hidden_units(total, down_ref.shape[0], width)
    out_ref[...] = dot(act, down_ref[...])[: out_ref.shape[0]]


def column_copies(weights, owner, size, buf, base):
    step = buf.shape[2]
    pairs = []
    for weight in weights:
        for i in range(size // step):
            cols = pl.ds(pl.multiple_of(owner * size + i * step, step), step)
            pairs.append((weight.at[:, cols], buf.at[base + len(pairs)]))
    return pairs


def expert_send_body(n_send, rows_ref, gain_ref, gate_ref, up_ref, *refs):
    send_refs, (lhs_ref, tail_ref, wide) = refs[:n_send], refs[n_send:]
    slots, width = lhs_ref.shape
    split = width // LANES
    size = gate_ref.shape[2]
    wide[...] = rows_ref[...].astype(F32)
    squares = jnp.zeros((slots, LANES), F32)
    for q in range(split):
        values = wide[pl.ds(q, slots, stride=split), :]
        squares = squares + values * values
        cols = slice(q * LANES, (q + 1) * LANES)
        lhs_ref[:, cols] = (values * gain_ref[:, cols]).astype(BF16)
    tail = squares_tail(jnp.sum(squares, axis=1, keepdims=True))
    tail_ref[...] = tail
    for k, send in enumerate(send_refs):
        send[:, :size] = dot(lhs_ref[...], gate_ref[k]).astype(BF16)
        send[:, size : 2 * size] = dot(lhs_ref[...], up_ref[k]).astype(BF16)
        send[:, 2 * size :] = tail.astype(BF16)


def expert_keep_body(lhs_ref, tail_ref, gate_hbm, up_hbm, keep_ref, buf, sems):
    size, step = (keep_ref.shape[1] - LANES) // 2, buf.shape[2]
    copies = start_copies(column_copies((gate_hbm, up_hbm), peer(0), size, buf, 0), sems)
    keep_ref[:, 2 * size :] = tail_ref[...]
    for i, copy in enumerate(copies):
        copy.wait()
        keep_ref[:, i * step : (i + 1) * step] = dot(lhs_ref[...], buf[i])


def expert_mid_body(width, keep_ref, *refs):
    recv_refs, out_ref = refs[:-1], refs[-1]
    total = keep_ref[...]
    for recv in recv_refs:
        total = total + recv[...].astype(F32)
    out_ref[...] = hidden_units(total, out_ref.shape[1], width)


def down_keep_body(act_ref, down_ref, acc_ref):
    acc_ref[...] = dot(act_ref[...], down_ref[shard(act_ref.shape[1], peer(0)), :])


def down_rest_body(acc_ref, down_ref, *refs):
    recv_refs, out_ref, wide = refs[:-2], refs[-2], refs[-1]
    slots, width = acc_ref.shape
    split = width // LANES
    n_tp = len(recv_refs) + 1
    for q in range(0, split, 2):
        cols = slice(q * LANES, (q + 2) * LANES)
        rows = acc_ref[:, cols]
        for step, recv in enumerate(recv_refs, 1):
            owner = shard(recv.shape[1], peer(n_tp - step))
            rows = rows + dot(recv[...], down_ref[owner, cols])
        wide[pl.ds(q, slots, stride=split), :] = rows[:, :LANES]
        wide[pl.ds(q + 1, slots, stride=split), :] = rows[:, LANES:]
    out_ref[...] = wide[...].astype(BF16)


def combine_body(back_ref, comb_ref, shared_ref, out_ref, wide):
    tok, width = out_ref.shape
    slots = comb_ref.shape[1]
    split = width // LANES
    wide[...] = back_ref[...].astype(F32)
    comb = comb_ref[...]
    high = comb.astype(BF16)
    rest = comb - high.astype(F32)
    mid = rest.astype(BF16)
    for q in range(0, split, 2):
        cols = slice(q * LANES, (q + 2) * LANES)
        values = jnp.concatenate(
            [
                wide[pl.ds(q, slots, stride=split), :].astype(BF16),
                wide[pl.ds(q + 1, slots, stride=split), :].astype(BF16),
            ],
            axis=1,
        )
        total = shared_ref[:, cols] + dot(mid, values) + dot(high, values)
        out_ref[:, cols] = total.astype(BF16)


def shift(value, step):
    size = lax.axis_size("tp")
    return lax.ppermute(value, "tp", [(i, (i + step) % size) for i in range(size)])


def experts_plain(arrived, gain, gate_w, up_w, down_w, slots, width):
    values = arrived.reshape(slots, width).astype(F32)
    total = lax.psum(jnp.sum(values * values, axis=1, keepdims=True), "tp")
    normed = values * lax.rsqrt(total / (width * lax.axis_size("tp")) + 1e-06) * gain
    rows = normed.astype(BF16)
    gate, up = (
        lax.psum_scatter(dot(rows, w), "tp", scatter_dimension=1, tiled=True)
        for w in (gate_w, up_w)
    )
    act = lax.all_gather((jax.nn.silu(gate) * up).astype(BF16), "tp", axis=1, tiled=True)
    return dot(act, down_w).astype(BF16).reshape(arrived.shape)


def experts(arrived, gain, gate_peer, up_peer, gate_w, up_w, down_w, slots, width):
    n_tp = lax.axis_size("tp")
    size = gate_w.shape[1] // n_tp
    sds = jax.ShapeDtypeStruct
    work = 4 * slots * width * size
    step = 2 * LANES if size % (2 * LANES) == 0 else LANES
    pieces = size // step

    def streamed(count):
        return [pltpu.VMEM((count, width, step), BF16), pltpu.SemaphoreType.DMA((count,))]

    *sends, lhs, tail = call(
        functools.partial(expert_send_body, n_tp - 1),
        "expert_send",
        tuple(sds((slots, 2 * size + LANES), BF16) for _ in range(n_tp - 1))
        + (sds((slots, width), BF16), sds((slots, LANES), F32)),
        [VMEM] * 4,
        [pltpu.VMEM(arrived.shape, F32)],
        work * (n_tp - 1),
    )(arrived, gain, gate_peer, up_peer)
    received = [shift(send, step) for step, send in enumerate(sends, 1)]
    keep = call(
        expert_keep_body,
        "expert_keep",
        sds((slots, 2 * size + LANES), F32),
        [VMEM] * 2 + [HBM] * 2,
        streamed(pieces * 2),
        work,
    )(lhs, tail, stored(gate_w), stored(up_w))
    act = call(
        functools.partial(expert_mid_body, width * n_tp),
        "expert_mid",
        sds((slots, size), BF16),
        [VMEM] * n_tp,
        (),
        10 * slots * size,
    )(keep, *received)
    acts = [shift(act, step) for step in range(1, n_tp)]
    acc = call(
        down_keep_body, "down_keep", sds((slots, width), F32), [VMEM] * 2, (), work // 2
    )(act, down_w)
    return call(
        down_rest_body,
        "down_rest",
        pltpu.VMEM(arrived.shape, BF16),
        [VMEM] * (n_tp + 1),
        [pltpu.VMEM(arrived.shape, F32)],
        work // 2 * (n_tp - 1),
    )(acc, down_w, *acts)


def local(
    tokens,
    norm_gain,
    routes,
    route_weights,
    expert_gate,
    expert_up,
    expert_down,
    shared_gate,
    shared_up,
    shared_down,
):
    tok, width = tokens.shape
    picks = routes.shape[1]
    n_tp, n_ep = lax.axis_size("tp"), lax.axis_size("ep")
    cap = max(2, tok * picks // n_ep + 1)
    slots = n_ep * cap
    split = width // LANES
    hidden = expert_gate.shape[2]
    tok_rows = -(-tok // 16) * 16
    cols = 2 * hidden + LANES
    sds = jax.ShapeDtypeStruct
    sem = pltpu.SemaphoreType.DMA

    def exchange(value):
        blocks = value.reshape(n_ep, cap * split, LANES)
        moved = lax.all_to_all(blocks, "ep", split_axis=0, concat_axis=0, tiled=True)
        return moved.reshape(slots * split, LANES)

    gate_w, up_w, down_w = expert_gate[0], expert_up[0], expert_down[0]
    gain = norm_gain.reshape(1, width)
    size = hidden // n_tp
    n_send = n_tp - 1 if size % LANES == 0 else 0
    part = sds((n_send, width, size), BF16)
    outgoing, comb, *peers = call(
        functools.partial(dispatch_body, cap, n_send),
        "dispatch",
        (sds((slots * split, LANES), BF16), sds((tok, slots), F32))
        + ((sds((1, width), F32), part, part) if n_send else ()),
        [HBM] * (6 if n_send else 3),
        [
            pltpu.VMEM((slots * split, LANES), F32),
            pltpu.VMEM((tok, width), BF16),
            pltpu.VMEM((picks, tok), jnp.int32),
            pltpu.VMEM((picks, tok), F32),
            sem((4 + 2 * n_send,)),
        ],
        2 * tok * slots * width,
    )(
        *map(stored, (tokens, routes.T, route_weights.T)),
        *(map(stored, (gain, gate_w, up_w)) if n_send else ()),
    )
    arrived = exchange(outgoing)
    if n_send:
        result = experts(arrived, *peers, gate_w, up_w, down_w, slots, width)
    else:
        result = experts_plain(arrived, gain, gate_w, up_w, down_w, slots, width)
    result, tokens, gain = lax.optimization_barrier((result, tokens, gain))
    back = exchange(result)
    shared_keep, shared_send, shared_down_w = call(
        shared_in_body,
        "shared_in",
        (sds((tok_rows, cols), F32), sds((tok_rows, cols), BF16))
        + (sds(shared_down.shape, BF16),),
        [HBM] * 5,
        [
            pltpu.VMEM((tok, width), BF16),
            pltpu.VMEM((1, width), F32),
            pltpu.VMEM(shared_gate.shape, BF16),
            pltpu.VMEM(shared_up.shape, BF16),
            sem((5,)),
        ],
        4 * 256 * width * hidden,
    )(*map(stored, (tokens, gain, shared_gate, shared_up, shared_down)))
    shared_received = [shift(shared_send, step) for step in range(1, n_tp)]
    shared_out = call(
        functools.partial(shared_out_body, width * n_tp),
        "shared_out",
        sds((tok, width), F32),
        [VMEM] * (n_tp + 1),
        (),
        2 * 128 * width * hidden,
    )(shared_keep, *shared_received, shared_down_w)
    return call(
        combine_body,
        "combine",
        sds((tok, width), BF16),
        [VMEM] * 3,
        [pltpu.VMEM((slots * split, LANES), F32)],
        6 * tok * slots * width,
    )(back, comb, shared_out)


def solution(mesh):
    placed = (
        P("ep", "tp"),
        P("tp"),
        P("ep", None),
        P("ep", None),
        P("ep", "tp", None),
        P("ep", "tp", None),
        P("ep", None, "tp"),
        P("tp", None),
        P("tp", None),
        P(None, "tp"),
    )
    return jax.shard_map(
        local, mesh=mesh, in_specs=placed, out_specs=P("ep", "tp"), check_vma=False
    )
```

```python
import functools

import jax
import jax.numpy as jnp
from jax import lax
from jax.experimental import pallas as pl
from jax.experimental.pallas import tpu as pltpu
from jax.sharding import PartitionSpec as P

F32 = jnp.float32
BF16 = jnp.bfloat16
LANES = 128
AHEAD = 10**12
VMEM = pl.BlockSpec(memory_space=pltpu.VMEM)
HBM = pl.BlockSpec(memory_space=pltpu.HBM)


def call(body, name, outs, ins, scratch=(), flops=0, limit=8):
    return pl.pallas_call(
        body,
        name=name,
        out_shape=outs,
        in_specs=list(ins),
        out_specs=jax.tree.map(lambda _: VMEM, outs),
        scratch_shapes=list(scratch),
        cost_estimate=pl.CostEstimate(flops=flops, bytes_accessed=0, transcendentals=0),
        compiler_params=pltpu.CompilerParams(vmem_limit_bytes=limit * 2**20),
    )


def stored(value):
    return pltpu.with_memory_space_constraint(value, pltpu.HBM)


def start_copies(pairs, sems):
    copies = [pltpu.make_async_copy(src, dst, sems.at[i]) for i, (src, dst) in enumerate(pairs)]
    for copy in copies:
        copy.start()
    return copies


def dot(a, b):
    return jnp.dot(a, b, preferred_element_type=F32)


def shard(size, index):
    return pl.ds(pl.multiple_of(index * size, size), size)


def peer(step):
    return lax.rem(lax.axis_index("tp") + step, lax.axis_size("tp"))


def dispatch_body(cap, tok_hbm, routes_hbm, weight_hbm, out_ref, comb_ref, *scratch):
    wide, tok_ref, routes_ref, weight_ref, sems = scratch
    copies = start_copies(
        ((routes_hbm, routes_ref), (weight_hbm, weight_ref), (tok_hbm, tok_ref)), sems
    )
    tok, width = tok_ref.shape
    picks = routes_ref.shape[0]
    slots = comb_ref.shape[1]
    split = width // LANES
    slot = lax.broadcasted_iota(jnp.int32, (slots, tok), 0)
    expert = jnp.floor((slot.astype(F32) + 0.5) * (1.0 / cap)).astype(jnp.int32)
    rank = (slot - expert * cap).astype(F32)
    row = lax.broadcasted_iota(jnp.int32, (tok, tok), 0)
    col = lax.broadcasted_iota(jnp.int32, (tok, tok), 1)
    earlier = jnp.where(row < col, 1.0, 0.0).astype(BF16)
    copies[0].wait()
    copies[1].wait()
    routes = routes_ref[...]
    weights = weight_ref[...]
    scaled = 2.5 * weights / jnp.sum(weights, axis=0, keepdims=True)
    named = jnp.zeros((slots, tok), F32)
    gain = jnp.zeros((slots, tok), F32)
    for k in range(picks):
        same = routes[k : k + 1, :] == expert
        named = jnp.where(same, 1.0, named)
        gain = jnp.where(same, scaled[k : k + 1, :], gain)
    before = dot(named.astype(BF16), earlier)
    hit = jnp.where(before == rank, named, 0.0)
    pick = hit.astype(BF16)
    copies[2].wait()
    for q in range(0, split, 2):
        rows = dot(pick, tok_ref[:, q * LANES : (q + 2) * LANES])
        wide[pl.ds(q, slots, stride=split), :] = rows[:, :LANES]
        wide[pl.ds(q + 1, slots, stride=split), :] = rows[:, LANES:]
    out_ref[...] = wide[...].astype(BF16)
    comb_ref[...] = jnp.transpose(hit * gain)


def squares_tail(total):
    lane = lax.broadcasted_iota(jnp.int32, (total.shape[0], LANES), 1)
    high = total.astype(BF16).astype(F32)
    return jnp.where(lane == 0, high, jnp.where(lane == 1, total - high, 0.0))


def shared_in_body(tok_ref, gain_ref, gate_ref, up_ref, keep_ref, send_ref):
    hidden = gate_ref.shape[1]
    tok = tok_ref.shape[0]
    keep_ref[...] = jnp.zeros_like(keep_ref)
    values = tok_ref[...].astype(F32)
    keep_ref[:tok, 2 * hidden :] = squares_tail(jnp.sum(values * values, axis=1, keepdims=True))
    rows = (values * gain_ref[...]).astype(BF16)
    keep_ref[:tok, :hidden] = dot(rows, gate_ref[...])
    keep_ref[:tok, hidden : 2 * hidden] = dot(rows, up_ref[...])
    send_ref[...] = keep_ref[...].astype(BF16)


def hidden_units(total, hidden, width):
    squares = jnp.sum(total[:, 2 * hidden :], axis=1, keepdims=True)
    scale = lax.rsqrt(squares / width + 1e-06)
    gate = total[:, :hidden] * scale
    up = total[:, hidden : 2 * hidden] * scale
    return (gate / (1.0 + jnp.exp(-gate)) * up).astype(BF16)


def shared_out_body(width, keep_ref, *refs):
    recv_refs, down_ref, out_ref = refs[:-2], refs[-2], refs[-1]
    total = keep_ref[...]
    for recv in recv_refs:
        total = total + recv[...].astype(F32)
    act = hidden_units(total, down_ref.shape[0], width)
    out_ref[...] = dot(act, down_ref[...])[: out_ref.shape[0]]


def expert_send_body(n_send, rows_ref, gain_ref, gate_ref, up_ref, *refs):
    send_refs, (lhs_ref, tail_ref, wide) = refs[:n_send], refs[n_send:]
    slots, width = lhs_ref.shape
    split = width // LANES
    wide[...] = rows_ref[...].astype(F32)
    squares = jnp.zeros((slots, LANES), F32)
    for q in range(split):
        values = wide[pl.ds(q, slots, stride=split), :]
        squares = squares + values * values
        cols = slice(q * LANES, (q + 1) * LANES)
        lhs_ref[:, cols] = (values * gain_ref[:, cols]).astype(BF16)
    tail = squares_tail(jnp.sum(squares, axis=1, keepdims=True))
    tail_ref[...] = tail
    for k, send in enumerate(send_refs, 1):
        size = (send.shape[1] - LANES) // 2
        cols = shard(size, peer(k))
        send[:, :size] = dot(lhs_ref[...], gate_ref[:, cols]).astype(BF16)
        send[:, size : 2 * size] = dot(lhs_ref[...], up_ref[:, cols]).astype(BF16)
        send[:, 2 * size :] = tail.astype(BF16)


def expert_keep_body(lhs_ref, tail_ref, gate_ref, up_ref, keep_ref):
    size = (keep_ref.shape[1] - LANES) // 2
    cols = shard(size, peer(0))
    keep_ref[:, :size] = dot(lhs_ref[...], gate_ref[:, cols])
    keep_ref[:, size : 2 * size] = dot(lhs_ref[...], up_ref[:, cols])
    keep_ref[:, 2 * size :] = tail_ref[...]


def expert_mid_body(width, keep_ref, *refs):
    recv_refs, out_ref = refs[:-1], refs[-1]
    total = keep_ref[...]
    for recv in recv_refs:
        total = total + recv[...].astype(F32)
    out_ref[...] = hidden_units(total, out_ref.shape[1], width)


def down_keep_body(act_ref, down_ref, acc_ref):
    acc_ref[...] = dot(act_ref[...], down_ref[shard(act_ref.shape[1], peer(0)), :])


def down_rest_body(acc_ref, down_ref, *refs):
    recv_refs, out_ref, wide = refs[:-2], refs[-2], refs[-1]
    slots, width = acc_ref.shape
    split = width // LANES
    n_tp = len(recv_refs) + 1
    for q in range(0, split, 2):
        cols = slice(q * LANES, (q + 2) * LANES)
        rows = acc_ref[:, cols]
        for step, recv in enumerate(recv_refs, 1):
            owner = shard(recv.shape[1], peer(n_tp - step))
            rows = rows + dot(recv[...], down_ref[owner, cols])
        wide[pl.ds(q, slots, stride=split), :] = rows[:, :LANES]
        wide[pl.ds(q + 1, slots, stride=split), :] = rows[:, LANES:]
    out_ref[...] = wide[...].astype(BF16)


def combine_body(back_ref, comb_ref, shared_ref, out_ref, wide):
    tok, width = out_ref.shape
    slots = comb_ref.shape[1]
    split = width // LANES
    wide[...] = back_ref[...].astype(F32)
    comb = comb_ref[...]
    high = comb.astype(BF16)
    rest = comb - high.astype(F32)
    mid = rest.astype(BF16)
    for q in range(0, split, 2):
        cols = slice(q * LANES, (q + 2) * LANES)
        values = jnp.concatenate(
            [
                wide[pl.ds(q, slots, stride=split), :].astype(BF16),
                wide[pl.ds(q + 1, slots, stride=split), :].astype(BF16),
            ],
            axis=1,
        )
        total = shared_ref[:, cols] + dot(mid, values) + dot(high, values)
        out_ref[:, cols] = total.astype(BF16)


def shift(value, step):
    size = lax.axis_size("tp")
    return lax.ppermute(value, "tp", [(i, (i + step) % size) for i in range(size)])


def experts_plain(arrived, gain, gate_w, up_w, down_w, slots, width):
    values = arrived.reshape(slots, width).astype(F32)
    total = lax.psum(jnp.sum(values * values, axis=1, keepdims=True), "tp")
    normed = values * lax.rsqrt(total / (width * lax.axis_size("tp")) + 1e-06) * gain
    rows = normed.astype(BF16)
    gate, up = (
        lax.psum_scatter(dot(rows, w), "tp", scatter_dimension=1, tiled=True)
        for w in (gate_w, up_w)
    )
    act = lax.all_gather((jax.nn.silu(gate) * up).astype(BF16), "tp", axis=1, tiled=True)
    return dot(act, down_w).astype(BF16).reshape(arrived.shape)


def local(
    tokens,
    norm_gain,
    routes,
    route_weights,
    expert_gate,
    expert_up,
    expert_down,
    shared_gate,
    shared_up,
    shared_down,
):
    tok, width = tokens.shape
    picks = routes.shape[1]
    n_tp, n_ep = lax.axis_size("tp"), lax.axis_size("ep")
    cap = max(2, tok * picks // n_ep + 1)
    slots = n_ep * cap
    split = width // LANES
    hidden = expert_gate.shape[2]
    size = hidden // n_tp
    tok_rows = -(-tok // 16) * 16
    cols = 2 * hidden + LANES
    sds = jax.ShapeDtypeStruct
    sem = pltpu.SemaphoreType.DMA
    wide = pltpu.VMEM((slots * split, LANES), F32)
    block = sds((slots * split, LANES), BF16)
    gain = norm_gain.reshape(1, width)
    gate_w, up_w, down_w = expert_gate[0], expert_up[0], expert_down[0]
    work = 4 * slots * width * size

    def exchange(value):
        blocks = value.reshape(n_ep, cap * split, LANES)
        moved = lax.all_to_all(blocks, "ep", split_axis=0, concat_axis=0, tiled=True)
        return moved.reshape(slots * split, LANES)

    def after(value, *others):
        return lax.optimization_barrier((value,) + others)

    def shared_in(tokens, gain):
        keep, send = call(
            shared_in_body,
            "shared_in",
            (sds((tok_rows, cols), F32), sds((tok_rows, cols), BF16)),
            [VMEM] * 4,
            (),
            4 * 128 * width * hidden,
        )(tokens, gain, shared_gate, shared_up)
        return keep, [shift(send, step) for step in range(1, n_tp)]

    def shared_out(keep, received):
        return call(
            functools.partial(shared_out_body, width * n_tp),
            "shared_out",
            sds((tok, width), F32),
            [VMEM] * (n_tp + 1),
            (),
            2 * 128 * width * hidden,
        )(keep, *received, shared_down)

    outgoing, comb = call(
        functools.partial(dispatch_body, cap),
        "dispatch",
        (block, sds((tok, slots), F32)),
        [HBM] * 3,
        [
            wide,
            pltpu.VMEM((tok, width), BF16),
            pltpu.VMEM((picks, tok), jnp.int32),
            pltpu.VMEM((picks, tok), F32),
            sem((3,)),
        ],
        AHEAD,
    )(*map(stored, (tokens, routes.T, route_weights.T)))
    arrived = exchange(outgoing)
    if size % LANES != 0:
        arrived, tokens, gain = after(arrived, tokens, gain)
        shared = shared_out(*shared_in(tokens, gain))
        result = experts_plain(arrived, gain, gate_w, up_w, down_w, slots, width)
    else:
        *sends, lhs, tail = call(
            functools.partial(expert_send_body, n_tp - 1),
            "expert_send",
            tuple(sds((slots, 2 * size + LANES), BF16) for _ in range(n_tp - 1))
            + (sds((slots, width), BF16), sds((slots, LANES), F32)),
            [VMEM] * 4,
            [wide],
            work * (n_tp - 1),
        )(arrived, gain, gate_w, up_w)
        received = [shift(send, step) for step, send in enumerate(sends, 1)]
        lhs, tokens, gain = after(lhs, tokens, gain)
        shared_keep, shared_received = shared_in(tokens, gain)
        keep = call(
            expert_keep_body,
            "expert_keep",
            sds((slots, 2 * size + LANES), F32),
            [VMEM] * 4,
            (),
            work,
        )(lhs, tail, gate_w, up_w)
        act = call(
            functools.partial(expert_mid_body, width * n_tp),
            "expert_mid",
            sds((slots, size), BF16),
            [VMEM] * n_tp,
            (),
            10 * slots * size,
        )(keep, *received)
        acts = [shift(act, step) for step in range(1, n_tp)]
        acc = call(
            down_keep_body, "down_keep", sds((slots, width), F32), [VMEM] * 2, (), work // 2
        )(act, down_w)
        shared = shared_out(shared_keep, shared_received)
        acc, shared = after(acc, shared)
        result = call(
            down_rest_body,
            "down_rest",
            block,
            [VMEM] * (n_tp + 1),
            [wide],
            work // 2 * (n_tp - 1),
        )(acc, down_w, *acts)
    result, shared = after(result, shared)
    back = exchange(result)
    return call(
        combine_body, "combine", sds((tok, width), BF16), [VMEM] * 3, [wide], AHEAD // 10**4
    )(back, comb, shared)


def solution(mesh):
    placed = (
        P("ep", "tp"),
        P("tp"),
        P("ep", None),
        P("ep", None),
        P("ep", "tp", None),
        P("ep", "tp", None),
        P("ep", None, "tp"),
        P("tp", None),
        P("tp", None),
        P(None, "tp"),
    )
    return jax.shard_map(
        local, mesh=mesh, in_specs=placed, out_specs=P("ep", "tp"), check_vma=False
    )
```

```python
import functools

import jax
import jax.numpy as jnp
from jax import lax
from jax.experimental import pallas as pl
from jax.experimental.pallas import tpu as pltpu
from jax.sharding import PartitionSpec as P


F32 = jnp.float32
BF16 = jnp.bfloat16
LANES = 128
N_HELD = 4
AHEAD = 10**12
VMEM = pl.BlockSpec(memory_space=pltpu.VMEM)
HBM = pl.BlockSpec(memory_space=pltpu.HBM)


def call(body, outs, ins, scratch=(), flops=0, limit=8):
    return pl.pallas_call(
        body,
        out_shape=outs,
        in_specs=list(ins),
        out_specs=jax.tree.map(lambda _: VMEM, outs),
        scratch_shapes=list(scratch),
        cost_estimate=pl.CostEstimate(flops=flops, bytes_accessed=0, transcendentals=0),
        compiler_params=pltpu.CompilerParams(vmem_limit_bytes=limit * 2**20),
    )


def stored(value):
    return pltpu.with_memory_space_constraint(value, pltpu.HBM)


def start_copies(pairs, sems):
    copies = [pltpu.make_async_copy(src, dst, sems.at[i]) for i, (src, dst) in enumerate(pairs)]
    for copy in copies:
        copy.start()
    return copies


def dot(a, b):
    return jnp.dot(a, b, preferred_element_type=F32)


def shard(size, index, chunk=0, chunks=1):
    part = size // chunks
    return pl.ds(pl.multiple_of(index * size + chunk * part, part), part)


def peer(step):
    return lax.rem(lax.axis_index("tp") + step, lax.axis_size("tp"))


def dispatch_body(cap, tok_hbm, routes_hbm, weight_hbm, out_ref, comb_ref, *scratch):
    wide, tok_ref, routes_ref, weight_ref, sems = scratch
    copies = start_copies(
        ((routes_hbm, routes_ref), (weight_hbm, weight_ref), (tok_hbm, tok_ref)), sems
    )
    tok, width = tok_ref.shape
    picks = routes_ref.shape[0]
    slots = comb_ref.shape[1]
    split = width // LANES
    slot = lax.broadcasted_iota(jnp.int32, (slots, tok), 0)
    expert = jnp.floor((slot.astype(F32) + 0.5) * (1.0 / cap)).astype(jnp.int32)
    rank = (slot - expert * cap).astype(F32)
    row = lax.broadcasted_iota(jnp.int32, (tok, tok), 0)
    col = lax.broadcasted_iota(jnp.int32, (tok, tok), 1)
    earlier = jnp.where(row < col, 1.0, 0.0).astype(BF16)
    copies[0].wait()
    copies[1].wait()
    routes = routes_ref[...]
    weights = weight_ref[...]
    scaled = 2.5 * weights / jnp.sum(weights, axis=0, keepdims=True)
    named = jnp.zeros((slots, tok), F32)
    gain = jnp.zeros((slots, tok), F32)
    for k in range(picks):
        same = routes[k : k + 1, :] == expert
        named = jnp.where(same, 1.0, named)
        gain = jnp.where(same, scaled[k : k + 1, :], gain)
    before = dot(named.astype(BF16), earlier)
    hit = jnp.where(before == rank, named, 0.0)
    pick = hit.astype(BF16)
    copies[2].wait()
    for q in range(0, split, 2):
        rows = dot(pick, tok_ref[:, q * LANES : (q + 2) * LANES])
        wide[pl.ds(q, slots, stride=split), :] = rows[:, :LANES]
        wide[pl.ds(q + 1, slots, stride=split), :] = rows[:, LANES:]
    out_ref[...] = wide[...].astype(BF16)
    comb_ref[...] = jnp.transpose(hit * gain)


def squares_tail(total):
    lane = lax.broadcasted_iota(jnp.int32, (total.shape[0], LANES), 1)
    high = total.astype(BF16).astype(F32)
    return jnp.where(lane == 0, high, jnp.where(lane == 1, total - high, 0.0))


def shared_in_body(tok_ref, gain_ref, gate_ref, up_ref, keep_ref, send_ref):
    hidden = gate_ref.shape[1]
    tok = tok_ref.shape[0]
    keep_ref[...] = jnp.zeros_like(keep_ref)
    values = tok_ref[...].astype(F32)
    keep_ref[:tok, 2 * hidden :] = squares_tail(jnp.sum(values * values, axis=1, keepdims=True))
    rows = (values * gain_ref[...]).astype(BF16)
    keep_ref[:tok, :hidden] = dot(rows, gate_ref[...])
    keep_ref[:tok, hidden : 2 * hidden] = dot(rows, up_ref[...])
    send_ref[...] = keep_ref[...].astype(BF16)


def row_scale(tail, width):
    return lax.rsqrt(jnp.sum(tail, axis=1, keepdims=True) / width + 1e-06)


def hidden_units(total, scale, hidden):
    gate = total[:, :hidden] * scale
    up = total[:, hidden : 2 * hidden] * scale
    return (gate / (1.0 + jnp.exp(-gate)) * up).astype(BF16)


def shared_out_body(width, keep_ref, *refs):
    recv_refs, down_ref, out_ref = refs[:-2], refs[-2], refs[-1]
    total = keep_ref[...]
    for recv in recv_refs:
        total = total + recv[...].astype(F32)
    hidden = down_ref.shape[0]
    act = hidden_units(total, row_scale(total[:, 2 * hidden :], width), hidden)
    out_ref[...] = dot(act, down_ref[...])[: out_ref.shape[0]]


def send_part(send, lhs_ref, gate_ref, up_ref, k, chunk, chunks):
    size = gate_ref.shape[1] // lax.axis_size("tp")
    part = size // chunks
    cols = shard(size, peer(k), chunk, chunks)
    send[:, :part] = dot(lhs_ref[...], gate_ref[:, cols]).astype(BF16)
    send[:, part : 2 * part] = dot(lhs_ref[...], up_ref[:, cols]).astype(BF16)


def expert_first_body(n_send, chunks, rows_ref, gain_ref, gate_ref, up_ref, *refs):
    refs = refs[N_HELD:]
    send_refs, (lhs_ref, tail_ref, wide) = refs[:n_send], refs[n_send:]
    slots, width = lhs_ref.shape
    split = width // LANES
    wide[...] = rows_ref[...].astype(F32)
    squares = jnp.zeros((slots, LANES), F32)
    for q in range(split):
        values = wide[pl.ds(q, slots, stride=split), :]
        squares = squares + values * values
        cols = slice(q * LANES, (q + 1) * LANES)
        lhs_ref[:, cols] = (values * gain_ref[:, cols]).astype(BF16)
    tail = squares_tail(jnp.sum(squares, axis=1, keepdims=True))
    tail_ref[...] = tail
    for k, send in enumerate(send_refs, 1):
        send_part(send, lhs_ref, gate_ref, up_ref, k, 0, chunks)
        send[:, -LANES:] = tail.astype(BF16)


def expert_later_body(chunk, chunks, lhs_ref, gate_ref, up_ref, *send_refs):
    for k, send in enumerate(send_refs, 1):
        send_part(send, lhs_ref, gate_ref, up_ref, k, chunk, chunks)


def expert_keep_body(lhs_ref, gate_ref, up_ref, *keep_refs):
    chunks = len(keep_refs)
    part = keep_refs[0].shape[1] // 2
    for chunk, keep in enumerate(keep_refs):
        cols = shard(part * chunks, peer(0), chunk, chunks)
        keep[:, :part] = dot(lhs_ref[...], gate_ref[:, cols])
        keep[:, part:] = dot(lhs_ref[...], up_ref[:, cols])


def first_mid_body(width, keep_ref, tail_ref, *refs):
    recv_refs, out_ref, scale_ref = refs[:-2], refs[-2], refs[-1]
    total, tail = keep_ref[...], tail_ref[...]
    part = out_ref.shape[1]
    for recv in recv_refs:
        total = total + recv[:, : 2 * part].astype(F32)
        tail = tail + recv[:, 2 * part :].astype(F32)
    scale = row_scale(tail, width)
    scale_ref[...] = jnp.broadcast_to(scale, scale_ref.shape)
    out_ref[...] = hidden_units(total, scale, part)


def later_mid_body(keep_ref, scale_ref, *refs):
    recv_refs, out_ref = refs[:-1], refs[-1]
    total = keep_ref[...]
    for recv in recv_refs:
        total = total + recv[...].astype(F32)
    out_ref[...] = hidden_units(total, scale_ref[:, :1], out_ref.shape[1])


def down_keep_body(down_ref, *refs):
    act_refs, acc_ref = refs[:-1], refs[-1]
    chunks = len(act_refs)
    size = act_refs[0].shape[1] * chunks
    act = jnp.concatenate([ref[...] for ref in act_refs], axis=1)
    acc_ref[...] = dot(act, down_ref[shard(size, peer(0)), :])


def down_rest_body(n_tp, acc_ref, down_ref, *refs):
    recv_refs, out_ref, wide = refs[:-2], refs[-2], refs[-1]
    slots, width = acc_ref.shape
    split = width // LANES
    chunks = len(recv_refs) // (n_tp - 1)
    size = recv_refs[0].shape[1] * chunks
    acts = []
    for step in range(1, n_tp):
        parts = recv_refs[(step - 1) * chunks : step * chunks]
        acts.append(jnp.concatenate([ref[...] for ref in parts], axis=1))
    for q in range(0, split, 2):
        cols = slice(q * LANES, (q + 2) * LANES)
        rows = acc_ref[:, cols]
        for step, act in enumerate(acts, 1):
            rows = rows + dot(act, down_ref[shard(size, peer(n_tp - step)), cols])
        wide[pl.ds(q, slots, stride=split), :] = rows[:, :LANES]
        wide[pl.ds(q + 1, slots, stride=split), :] = rows[:, LANES:]
    out_ref[...] = wide[...].astype(BF16)


def combine_body(back_ref, comb_ref, shared_ref, out_ref, wide):
    _, width = out_ref.shape
    slots = comb_ref.shape[1]
    split = width // LANES
    wide[...] = back_ref[...].astype(F32)
    comb = comb_ref[...]
    high = comb.astype(BF16)
    rest = comb - high.astype(F32)
    mid = rest.astype(BF16)
    for q in range(0, split, 2):
        cols = slice(q * LANES, (q + 2) * LANES)
        values = jnp.concatenate(
            [
                wide[pl.ds(q, slots, stride=split), :].astype(BF16),
                wide[pl.ds(q + 1, slots, stride=split), :].astype(BF16),
            ],
            axis=1,
        )
        total = shared_ref[:, cols] + dot(mid, values) + dot(high, values)
        out_ref[:, cols] = total.astype(BF16)


def shift(value, step):
    size = lax.axis_size("tp")
    return lax.ppermute(value, "tp", [(i, (i + step) % size) for i in range(size)])


def experts_plain(arrived, gain, gate_w, up_w, down_w, slots, width):
    values = arrived.reshape(slots, width).astype(F32)
    total = lax.psum(jnp.sum(values * values, axis=1, keepdims=True), "tp")
    normed = values * lax.rsqrt(total / (width * lax.axis_size("tp")) + 1e-06) * gain
    rows = normed.astype(BF16)
    gate, up = (
        lax.psum_scatter(dot(rows, w), "tp", scatter_dimension=1, tiled=True)
        for w in (gate_w, up_w)
    )
    act = lax.all_gather((jax.nn.silu(gate) * up).astype(BF16), "tp", axis=1, tiled=True)
    return dot(act, down_w).astype(BF16).reshape(arrived.shape)


def local(
    tokens,
    norm_gain,
    routes,
    route_weights,
    expert_gate,
    expert_up,
    expert_down,
    shared_gate,
    shared_up,
    shared_down,
):
    tok, width = tokens.shape
    picks = routes.shape[1]
    n_tp, n_ep = lax.axis_size("tp"), lax.axis_size("ep")
    cap = max(2, tok * picks // n_ep + 1)
    slots = n_ep * cap
    split = width // LANES
    hidden = expert_gate.shape[2]
    size = hidden // n_tp
    tok_rows = -(-tok // 16) * 16
    cols = 2 * hidden + LANES
    sds = jax.ShapeDtypeStruct
    sem = pltpu.SemaphoreType.DMA
    wide = pltpu.VMEM((slots * split, LANES), F32)
    block = sds((slots * split, LANES), BF16)
    gain = norm_gain.reshape(1, width)
    gate_w, up_w, down_w = expert_gate[0], expert_up[0], expert_down[0]
    work = 4 * slots * width * size

    def exchange(value):
        blocks = value.reshape(n_ep, cap * split, LANES)
        moved = lax.all_to_all(blocks, "ep", split_axis=0, concat_axis=0, tiled=True)
        return moved.reshape(slots * split, LANES)

    def after(value, *others):
        return lax.optimization_barrier((value,) + others)

    def shared_in(tokens, gain):
        keep, send = call(
            shared_in_body,
            (sds((tok_rows, cols), F32), sds((tok_rows, cols), BF16)),
            [VMEM] * 4,
            (),
            4 * 128 * width * hidden,
        )(tokens, gain, shared_gate, shared_up)
        return keep, [shift(send, step) for step in range(1, n_tp)]

    def shared_out(keep, received):
        return call(
            functools.partial(shared_out_body, width * n_tp),
            sds((tok, width), F32),
            [VMEM] * (n_tp + 1),
            (),
            2 * 128 * width * hidden,
        )(keep, *received, shared_down)

    outgoing, comb = call(
        functools.partial(dispatch_body, cap),
        (block, sds((tok, slots), F32)),
        [HBM] * 3,
        [
            wide,
            pltpu.VMEM((tok, width), BF16),
            pltpu.VMEM((picks, tok), jnp.int32),
            pltpu.VMEM((picks, tok), F32),
            sem((3,)),
        ],
        AHEAD,
    )(*map(stored, (tokens, routes.T, route_weights.T)))
    arrived = exchange(outgoing)
    if size % LANES != 0:
        arrived, tokens, gain = after(arrived, tokens, gain)
        shared_keep, shared_received = shared_in(tokens, gain)
        result = experts_plain(arrived, gain, gate_w, up_w, down_w, slots, width)
    else:
        chunks = 2 if size % (2 * LANES) == 0 else 1
        part = size // chunks
        n_send = n_tp - 1

        def sends(extra):
            return tuple(sds((slots, 2 * part + extra), BF16) for _ in range(n_send))

        def shifted(values):
            return [shift(value, step) for step, value in enumerate(values, 1)]

        *sent, lhs, tail = call(
            functools.partial(expert_first_body, n_send, chunks),
            sends(LANES) + (sds((slots, width), BF16), sds((slots, LANES), F32)),
            [VMEM] * (4 + N_HELD),
            [wide],
            work * n_send // chunks,
        )(arrived, gain, gate_w, up_w, shared_gate, shared_up, down_w, shared_down)
        received = [shifted(sent)]
        for chunk in range(1, chunks):
            sent = call(
                functools.partial(expert_later_body, chunk, chunks),
                sends(0),
                [VMEM] * 3,
                (),
                work * n_send // chunks,
            )(lhs, gate_w, up_w)
            lhs, *sent = after(lhs, *sent)
            received.append(shifted(sent))
        keeps = call(
            expert_keep_body,
            (sds((slots, 2 * part), F32),) * chunks,
            [VMEM] * 3,
            (),
            work,
        )(lhs, gate_w, up_w)
        lhs, tokens, gain = after(lhs, tokens, gain)
        shared_keep, shared_received = shared_in(tokens, gain)
        act, scale = call(
            functools.partial(first_mid_body, width * n_tp),
            (sds((slots, part), BF16), sds((slots, LANES), F32)),
            [VMEM] * (n_tp + 1),
            (),
            10 * slots * part,
        )(keeps[0], tail, *received[0])
        own = [act]
        acts = [[shift(act, step)] for step in range(1, n_tp)]
        for chunk in range(1, chunks):
            act = call(
                later_mid_body,
                sds((slots, part), BF16),
                [VMEM] * (n_tp + 1),
                (),
                10 * slots * part,
            )(keeps[chunk], scale, *received[chunk])
            own.append(act)
            for step in range(1, n_tp):
                acts[step - 1].append(shift(act, step))
        acc = call(
            down_keep_body,
            sds((slots, width), F32),
            [VMEM] * (chunks + 1),
            (),
            work // 2,
        )(down_w, *own)
        result = call(
            functools.partial(down_rest_body, n_tp),
            block,
            [VMEM] * (2 + chunks * n_send),
            [wide],
            work // 2 * n_send,
        )(acc, down_w, *(act for parts in acts for act in parts))
    shared = shared_out(shared_keep, shared_received)
    result, shared = after(result, shared)
    back = exchange(result)
    return call(
        combine_body, sds((tok, width), BF16), [VMEM] * 3, [wide], AHEAD // 10**4
    )(back, comb, shared)


def solution(mesh):
    placed = (
        P("ep", "tp"),
        P("tp"),
        P("ep", None),
        P("ep", None),
        P("ep", "tp", None),
        P("ep", "tp", None),
        P("ep", None, "tp"),
        P("tp", None),
        P("tp", None),
        P(None, "tp"),
    )

    return jax.shard_map(
        local, mesh=mesh, in_specs=placed, out_specs=P("ep", "tp"), check_vma=False
    )
```

```python
import functools

import jax
import jax.numpy as jnp
from jax import lax
from jax.experimental import pallas as pl
from jax.experimental.pallas import tpu as pltpu
from jax.sharding import PartitionSpec as P


F32 = jnp.float32
BF16 = jnp.bfloat16
LANES = 128
N_HELD = 4
AHEAD = 10**12
VMEM = pl.BlockSpec(memory_space=pltpu.VMEM)
HBM = pl.BlockSpec(memory_space=pltpu.HBM)


def call(body, outs, ins, scratch=(), flops=0, limit=8):
    return pl.pallas_call(
        body,
        out_shape=outs,
        in_specs=list(ins),
        out_specs=jax.tree.map(lambda _: VMEM, outs),
        scratch_shapes=list(scratch),
        cost_estimate=pl.CostEstimate(flops=flops, bytes_accessed=0, transcendentals=0),
        compiler_params=pltpu.CompilerParams(vmem_limit_bytes=limit * 2**20),
    )


def stored(value):
    return pltpu.with_memory_space_constraint(value, pltpu.HBM)


def start_copies(pairs, sems):
    copies = [pltpu.make_async_copy(src, dst, sems.at[i]) for i, (src, dst) in enumerate(pairs)]
    for copy in copies:
        copy.start()
    return copies


def dot(a, b):
    return jnp.dot(a, b, preferred_element_type=F32)


def shard(size, index, chunk=0, chunks=1):
    part = size // chunks
    return pl.ds(pl.multiple_of(index * size + chunk * part, part), part)


def peer(step):
    return lax.rem(lax.axis_index("tp") + step, lax.axis_size("tp"))


def dispatch_body(cap, tok_hbm, routes_hbm, weight_hbm, out_ref, comb_ref, *scratch):
    wide, tok_ref, routes_ref, weight_ref, sems = scratch
    copies = start_copies(
        ((routes_hbm, routes_ref), (weight_hbm, weight_ref), (tok_hbm, tok_ref)), sems
    )
    tok, width = tok_ref.shape
    picks = routes_ref.shape[0]
    slots = comb_ref.shape[1]
    split = width // LANES
    slot = lax.broadcasted_iota(jnp.int32, (slots, tok), 0)
    expert = jnp.floor((slot.astype(F32) + 0.5) * (1.0 / cap)).astype(jnp.int32)
    rank = (slot - expert * cap).astype(F32)
    row = lax.broadcasted_iota(jnp.int32, (tok, tok), 0)
    col = lax.broadcasted_iota(jnp.int32, (tok, tok), 1)
    earlier = jnp.where(row < col, 1.0, 0.0).astype(BF16)
    copies[0].wait()
    copies[1].wait()
    routes = routes_ref[...]
    weights = weight_ref[...]
    scaled = 2.5 * weights / jnp.sum(weights, axis=0, keepdims=True)
    named = jnp.zeros((slots, tok), F32)
    gain = jnp.zeros((slots, tok), F32)
    for k in range(picks):
        same = routes[k : k + 1, :] == expert
        named = jnp.where(same, 1.0, named)
        gain = jnp.where(same, scaled[k : k + 1, :], gain)
    before = dot(named.astype(BF16), earlier)
    hit = jnp.where(before == rank, named, 0.0)
    pick = hit.astype(BF16)
    copies[2].wait()
    for q in range(0, split, 2):
        rows = dot(pick, tok_ref[:, q * LANES : (q + 2) * LANES])
        wide[pl.ds(q, slots, stride=split), :] = rows[:, :LANES]
        wide[pl.ds(q + 1, slots, stride=split), :] = rows[:, LANES:]
    out_ref[...] = wide[...].astype(BF16)
    comb_ref[...] = jnp.transpose(hit * gain)


def squares_tail(total):
    lane = lax.broadcasted_iota(jnp.int32, (total.shape[0], LANES), 1)
    high = jnp.minimum(total, 3.3e38).astype(BF16).astype(F32)
    return jnp.where(lane == 0, high, jnp.where(lane == 1, total - high, 0.0))


def shared_in_body(tok_ref, gain_ref, gate_ref, up_ref, keep_ref, send_ref):
    hidden = gate_ref.shape[1]
    tok = tok_ref.shape[0]
    keep_ref[...] = jnp.zeros_like(keep_ref)
    values = tok_ref[...].astype(F32)
    keep_ref[:tok, 2 * hidden :] = squares_tail(jnp.sum(values * values, axis=1, keepdims=True))
    rows = (values * gain_ref[...]).astype(BF16)
    keep_ref[:tok, :hidden] = dot(rows, gate_ref[...])
    keep_ref[:tok, hidden : 2 * hidden] = dot(rows, up_ref[...])
    send_ref[...] = keep_ref[...].astype(BF16)


def row_scale(tail, width):
    return lax.rsqrt(jnp.sum(tail, axis=1, keepdims=True) / width + 1e-06)


def hidden_units(total, scale, hidden):
    alive = scale > 0.0
    gate = jnp.where(alive, total[:, :hidden] * scale, 0.0)
    up = jnp.where(alive, total[:, hidden : 2 * hidden] * scale, 0.0)
    return (gate / (1.0 + jnp.exp(-gate)) * up).astype(BF16)


def shared_out_body(width, keep_ref, *refs):
    recv_refs, down_ref, out_ref = refs[:-2], refs[-2], refs[-1]
    total = keep_ref[...]
    for recv in recv_refs:
        total = total + recv[...].astype(F32)
    hidden = down_ref.shape[0]
    act = hidden_units(total, row_scale(total[:, 2 * hidden :], width), hidden)
    out_ref[...] = dot(act, down_ref[...])[: out_ref.shape[0]]


def send_part(send, lhs_ref, gate_ref, up_ref, k, chunk, chunks):
    size = gate_ref.shape[1] // lax.axis_size("tp")
    part = size // chunks
    cols = shard(size, peer(k), chunk, chunks)
    send[:, :part] = dot(lhs_ref[...], gate_ref[:, cols]).astype(BF16)
    send[:, part : 2 * part] = dot(lhs_ref[...], up_ref[:, cols]).astype(BF16)


def expert_first_body(n_send, chunks, rows_ref, gain_ref, gate_ref, up_ref, *refs):
    refs = refs[N_HELD:]
    send_refs, (lhs_ref, tail_ref, wide) = refs[:n_send], refs[n_send:]
    slots, width = lhs_ref.shape
    split = width // LANES
    wide[...] = rows_ref[...].astype(F32)
    squares = jnp.zeros((slots, LANES), F32)
    for q in range(split):
        values = wide[pl.ds(q, slots, stride=split), :]
        squares = squares + values * values
        cols = slice(q * LANES, (q + 1) * LANES)
        lhs_ref[:, cols] = (values * gain_ref[:, cols]).astype(BF16)
    tail = squares_tail(jnp.sum(squares, axis=1, keepdims=True))
    tail_ref[...] = tail
    for k, send in enumerate(send_refs, 1):
        send_part(send, lhs_ref, gate_ref, up_ref, k, 0, chunks)
        send[:, -LANES:] = tail.astype(BF16)


def expert_later_body(chunk, chunks, lhs_ref, gate_ref, up_ref, *send_refs):
    for k, send in enumerate(send_refs, 1):
        send_part(send, lhs_ref, gate_ref, up_ref, k, chunk, chunks)


def expert_keep_body(lhs_ref, gate_ref, up_ref, *keep_refs):
    chunks = len(keep_refs)
    part = keep_refs[0].shape[1] // 2
    for chunk, keep in enumerate(keep_refs):
        cols = shard(part * chunks, peer(0), chunk, chunks)
        keep[:, :part] = dot(lhs_ref[...], gate_ref[:, cols])
        keep[:, part:] = dot(lhs_ref[...], up_ref[:, cols])


def first_mid_body(width, keep_ref, tail_ref, *refs):
    recv_refs, out_ref, scale_ref = refs[:-2], refs[-2], refs[-1]
    total, tail = keep_ref[...], tail_ref[...]
    part = out_ref.shape[1]
    for recv in recv_refs:
        total = total + recv[:, : 2 * part].astype(F32)
        tail = tail + recv[:, 2 * part :].astype(F32)
    scale = row_scale(tail, width)
    scale_ref[...] = jnp.broadcast_to(scale, scale_ref.shape)
    out_ref[...] = hidden_units(total, scale, part)


def later_mid_body(keep_ref, scale_ref, *refs):
    recv_refs, out_ref = refs[:-1], refs[-1]
    total = keep_ref[...]
    for recv in recv_refs:
        total = total + recv[...].astype(F32)
    out_ref[...] = hidden_units(total, scale_ref[:, :1], out_ref.shape[1])


def down_keep_body(down_ref, *refs):
    act_refs, acc_ref = refs[:-1], refs[-1]
    chunks = len(act_refs)
    size = act_refs[0].shape[1] * chunks
    act = jnp.concatenate([ref[...] for ref in act_refs], axis=1)
    acc_ref[...] = dot(act, down_ref[shard(size, peer(0)), :])


def down_rest_body(n_tp, acc_ref, down_ref, *refs):
    recv_refs, out_ref, wide = refs[:-2], refs[-2], refs[-1]
    slots, width = acc_ref.shape
    split = width // LANES
    chunks = len(recv_refs) // (n_tp - 1)
    size = recv_refs[0].shape[1] * chunks
    acts = []
    for step in range(1, n_tp):
        parts = recv_refs[(step - 1) * chunks : step * chunks]
        acts.append(jnp.concatenate([ref[...] for ref in parts], axis=1))
    for q in range(0, split, 2):
        cols = slice(q * LANES, (q + 2) * LANES)
        rows = acc_ref[:, cols]
        for step, act in enumerate(acts, 1):
            rows = rows + dot(act, down_ref[shard(size, peer(n_tp - step)), cols])
        wide[pl.ds(q, slots, stride=split), :] = rows[:, :LANES]
        wide[pl.ds(q + 1, slots, stride=split), :] = rows[:, LANES:]
    out_ref[...] = wide[...].astype(BF16)


def combine_body(back_ref, comb_ref, shared_ref, out_ref, wide):
    _, width = out_ref.shape
    slots = comb_ref.shape[1]
    split = width // LANES
    wide[...] = back_ref[...].astype(F32)
    comb = comb_ref[...]
    high = comb.astype(BF16)
    rest = comb - high.astype(F32)
    mid = rest.astype(BF16)
    for q in range(0, split, 2):
        cols = slice(q * LANES, (q + 2) * LANES)
        values = jnp.concatenate(
            [
                wide[pl.ds(q, slots, stride=split), :].astype(BF16),
                wide[pl.ds(q + 1, slots, stride=split), :].astype(BF16),
            ],
            axis=1,
        )
        total = shared_ref[:, cols] + dot(mid, values) + dot(high, values)
        out_ref[:, cols] = total.astype(BF16)


def shift(value, step):
    size = lax.axis_size("tp")
    return lax.ppermute(value, "tp", [(i, (i + step) % size) for i in range(size)])


def experts_plain(arrived, gain, gate_w, up_w, down_w, slots, width):
    values = arrived.reshape(slots, width).astype(F32)
    total = lax.psum(jnp.sum(values * values, axis=1, keepdims=True), "tp")
    normed = values * lax.rsqrt(total / (width * lax.axis_size("tp")) + 1e-06) * gain
    rows = normed.astype(BF16)
    gate, up = (
        lax.psum_scatter(dot(rows, w), "tp", scatter_dimension=1, tiled=True)
        for w in (gate_w, up_w)
    )
    act = lax.all_gather((jax.nn.silu(gate) * up).astype(BF16), "tp", axis=1, tiled=True)
    return dot(act, down_w).astype(BF16).reshape(arrived.shape)


def local(
    tokens,
    norm_gain,
    routes,
    route_weights,
    expert_gate,
    expert_up,
    expert_down,
    shared_gate,
    shared_up,
    shared_down,
):
    tok, width = tokens.shape
    picks = routes.shape[1]
    n_tp, n_ep = lax.axis_size("tp"), lax.axis_size("ep")
    cap = max(2, tok * picks // n_ep + 1)
    slots = n_ep * cap
    split = width // LANES
    hidden = expert_gate.shape[2]
    size = hidden // n_tp
    tok_rows = -(-tok // 16) * 16
    cols = 2 * hidden + LANES
    sds = jax.ShapeDtypeStruct
    sem = pltpu.SemaphoreType.DMA
    wide = pltpu.VMEM((slots * split, LANES), F32)
    block = sds((slots * split, LANES), BF16)
    gain = norm_gain.reshape(1, width)
    gate_w, up_w, down_w = expert_gate[0], expert_up[0], expert_down[0]
    work = 4 * slots * width * size

    def exchange(value):
        blocks = value.reshape(n_ep, cap * split, LANES)
        moved = lax.all_to_all(blocks, "ep", split_axis=0, concat_axis=0, tiled=True)
        return moved.reshape(slots * split, LANES)

    def after(value, *others):
        return lax.optimization_barrier((value,) + others)

    def shared_in(tokens, gain):
        keep, send = call(
            shared_in_body,
            (sds((tok_rows, cols), F32), sds((tok_rows, cols), BF16)),
            [VMEM] * 4,
            (),
            4 * 128 * width * hidden,
        )(tokens, gain, shared_gate, shared_up)
        return keep, [shift(send, step) for step in range(1, n_tp)]

    def shared_out(keep, received):
        return call(
            functools.partial(shared_out_body, width * n_tp),
            sds((tok, width), F32),
            [VMEM] * (n_tp + 1),
            (),
            2 * 128 * width * hidden,
        )(keep, *received, shared_down)

    outgoing, comb = call(
        functools.partial(dispatch_body, cap),
        (block, sds((tok, slots), F32)),
        [HBM] * 3,
        [
            wide,
            pltpu.VMEM((tok, width), BF16),
            pltpu.VMEM((picks, tok), jnp.int32),
            pltpu.VMEM((picks, tok), F32),
            sem((3,)),
        ],
        AHEAD,
    )(*map(stored, (tokens, routes.T, route_weights.T)))
    arrived = exchange(outgoing)
    if size % LANES != 0:
        arrived, tokens, gain = after(arrived, tokens, gain)
        shared_keep, shared_received = shared_in(tokens, gain)
        result = experts_plain(arrived, gain, gate_w, up_w, down_w, slots, width)
    else:
        chunks = 2 if size % (2 * LANES) == 0 else 1
        part = size // chunks
        n_send = n_tp - 1

        def sends(extra):
            return tuple(sds((slots, 2 * part + extra), BF16) for _ in range(n_send))

        def shifted(values):
            return [shift(value, step) for step, value in enumerate(values, 1)]

        *sent, lhs, tail = call(
            functools.partial(expert_first_body, n_send, chunks),
            sends(LANES) + (sds((slots, width), BF16), sds((slots, LANES), F32)),
            [VMEM] * (4 + N_HELD),
            [wide],
            work * n_send // chunks,
        )(arrived, gain, gate_w, up_w, shared_gate, shared_up, down_w, shared_down)
        received = [shifted(sent)]
        for chunk in range(1, chunks):
            sent = call(
                functools.partial(expert_later_body, chunk, chunks),
                sends(0),
                [VMEM] * 3,
                (),
                work * n_send // chunks,
            )(lhs, gate_w, up_w)
            lhs, *sent = after(lhs, *sent)
            received.append(shifted(sent))
        keeps = call(
            expert_keep_body,
            (sds((slots, 2 * part), F32),) * chunks,
            [VMEM] * 3,
            (),
            work,
        )(lhs, gate_w, up_w)
        lhs, tokens, gain = after(lhs, tokens, gain)
        shared_keep, shared_received = shared_in(tokens, gain)
        act, scale = call(
            functools.partial(first_mid_body, width * n_tp),
            (sds((slots, part), BF16), sds((slots, LANES), F32)),
            [VMEM] * (n_tp + 1),
            (),
            10 * slots * part,
        )(keeps[0], tail, *received[0])
        own = [act]
        acts = [[shift(act, step)] for step in range(1, n_tp)]
        for chunk in range(1, chunks):
            act = call(
                later_mid_body,
                sds((slots, part), BF16),
                [VMEM] * (n_tp + 1),
                (),
                10 * slots * part,
            )(keeps[chunk], scale, *received[chunk])
            own.append(act)
            for step in range(1, n_tp):
                acts[step - 1].append(shift(act, step))
        acc = call(
            down_keep_body,
            sds((slots, width), F32),
            [VMEM] * (chunks + 1),
            (),
            work // 2,
        )(down_w, *own)
        result = call(
            functools.partial(down_rest_body, n_tp),
            block,
            [VMEM] * (2 + chunks * n_send),
            [wide],
            work // 2 * n_send,
        )(acc, down_w, *(act for parts in acts for act in parts))
    shared = shared_out(shared_keep, shared_received)
    result, shared = after(result, shared)
    back = exchange(result)
    return call(
        combine_body, sds((tok, width), BF16), [VMEM] * 3, [wide], AHEAD // 10**4
    )(back, comb, shared)


def solution(mesh):
    placed = (
        P("ep", "tp"),
        P("tp"),
        P("ep", None),
        P("ep", None),
        P("ep", "tp", None),
        P("ep", "tp", None),
        P("ep", None, "tp"),
        P("tp", None),
        P("tp", None),
        P(None, "tp"),
    )

    return jax.shard_map(
        local, mesh=mesh, in_specs=placed, out_specs=P("ep", "tp"), check_vma=False
    )
```
